32 devices in a mesh: ep: 8 (over z, core), tp: 4 (over y, x).
Axes of the slice: x: 2, y: 2, z: 4, core: 2. Of those that a mesh axis runs over, the one named last changes fastest.
Arguments:
- tokens: bfloat16 [512, 2048], P('ep', 'tp'), may hold values from -6 to 6
- gain_mix: float32 [2048], replicated, may hold values from 0.1 to 1.9
- w_in: bfloat16 [2048, 1024], P(None, 'tp'), may hold values from -0.125 to 0.125
- decay_rate: float32 [64, 64], P('tp'), may hold values from 0.05 to 3
- frequency: float32 [64, 64], P('tp'), may hold values from -3 to 3
- log_step: float32 [64], P('tp'), may hold values from -3 to 0
- input_real: float32 [64, 64, 16], P('tp'), may hold values from -1 to 1
- input_imag: float32 [64, 64, 16], P('tp'), may hold values from -1 to 1
- readout_real: float32 [64, 16, 64], P('tp'), may hold values from -0.75 to 0.75
- readout_imaginary: float32 [64, 16, 64], P('tp'), may hold values from -0.75 to 0.75
- passthrough_scale: float32 [1024], P('tp'), may hold values from -4 to 4
- state_real: float32 [512, 64, 64], P('ep', 'tp'), may hold values from -4 to 4
- state_imag: float32 [512, 64, 64], P('ep', 'tp'), may hold values from -4 to 4
- w_out: bfloat16 [1024, 2048], replicated, may hold values from -0.1875 to 0.1875
- gain_ffn: float32 [2048], replicated, may hold values from 0.1 to 1.9
- expert_choice: int32 [512, 2], P('ep'), may hold values from 0 to 7, all different within a row; in each aligned block of 64 rows (0 to 63, 64 to 127, ...) at most 32 rows name the same one
- expert_weight: float32 [512, 2], P('ep'), may hold values from 0.2 to 1
- w_gate: bfloat16 [8, 2048, 8192], P('ep', None, 'tp'), may hold values from -0.125 to 0.125
- w_up: bfloat16 [8, 2048, 8192], P('ep', None, 'tp'), may hold values from -0.125 to 0.125
- w_down: bfloat16 [8, 8192, 2048], P('ep', 'tp'), may hold values from -0.0625 to 0.0625
Outputs:
- layer_out: bfloat16 [512, 2048], P('ep', 'tp')
- next_state_real: float32 [512, 64, 64], P('ep', 'tp')
- next_state_imaginary: float32 [512, 64, 64], P('ep', 'tp')
The draws below stay inside these ranges and needn't reach their ends.
Inputs may be any that keep to these rules, and one draw needn't show every extreme that they name: `expert_choice`: each row names 2 different experts; in the rows of one index of ep (aligned blocks of 64 rows) no expert is named more than 32 times, a bound that some block reaches.
All inputs are finite; a program needn't handle non-finite values.
Results may differ from the reference program's by a relative error of at most 0.017.
Values may be sent and summed in bfloat16 or wider, within the bound.
A program may use at most 64 MiB of HBM per device.

```python
import math
import jax
import jax.numpy as jnp
import numpy as np
from jax import lax

D = 2048
SSM_WIDTH = 1024
CHANNELS = 16
STATE = 64
FF = 8192
TOP = 2
SEQS = 64
GROUPS = 64
EXPERTS = 8
CAP = 32
ROWS = 512
N_EP = 8
N_TP = 4


def level_of(own_key, shape, shards, low, high):
    def one(position, shards_of):
        heights = jax.random.uniform(jax.random.fold_in(jax.random.fold_in(own_key, 6), position), (shards_of,), jnp.float32, low / len(shards), high / len(shards))
        return jnp.repeat(jnp.exp(heights), shape[position] // shards_of).reshape((-1,) + (1,) * (len(shape) - position - 1))

    level = one(*shards[0])
    for cut in shards[1:]:
        level = level * one(*cut)
    return level


def shared_out(stream_key, own, number, rows, number_of, top, reach, slope):
    ranking = jax.random.permutation(stream_key, number_of)
    heavy_load, common = shares(number_of, rows * top, reach, slope, True), shares(number_of, rows * top, reach, slope, False)
    places = jnp.arange(number_of)

    def named(tallies, offset_by):
        used = int((tallies > 0).sum())
        fixed = max(1, used // 4)
        passed = fixed + (places - fixed + offset_by * (used - fixed)) % max(1, number_of - fixed)
        return jnp.zeros((number_of,), jnp.int32).at[ranking[jnp.where(places < fixed, places, passed)]].set(jnp.asarray(tallies, jnp.int32))

    tallies = jnp.where(number % 4 == 0, named(heavy_load, number // 4), named(common, number - number // 4 - 1))
    mixed = jax.random.permutation(jax.random.fold_in(own, 3), number_of)
    donor, receiver = mixed[0:number_of // 2 * 2:2], mixed[1:number_of // 2 * 2:2]
    slack = jnp.minimum(tallies[donor] - 1, reach - tallies[receiver]) // 2
    slack = jnp.where((donor == ranking[0]) | (receiver == ranking[0]) | (tallies[receiver] == 0), 0, jnp.maximum(slack, 0))
    passed = jax.random.randint(jax.random.fold_in(own, 4), (number_of // 2,), 0, 1 << 20) % (slack + 1)
    tallies = tallies.at[donor].add(-passed).at[receiver].add(passed)
    members = jnp.searchsorted(jnp.cumsum(tallies), jnp.arange(rows * top), side="right").astype(jnp.int32)
    listing = members.reshape(top, rows).T
    listing = listing[jax.random.permutation(jax.random.fold_in(own, 1), rows)]
    offset_by = jax.random.randint(jax.random.fold_in(own, 2), (rows, 1), 0, top)
    return jnp.take_along_axis(listing, (jnp.arange(top)[None, :] + offset_by) % top, axis=1)


def shares(number_of, total, most, slope, full):
    weights = [(1 << 20) // math.isqrt(standing ** slope) + 1 for standing in range(1, number_of + 1)]
    largest = most if full else min(most, max(-(-total // number_of), total * weights[0] // sum(weights)))
    least = 1 if total - largest >= number_of - 1 else 0
    given, spare = [largest] + [least] * (number_of - 1), total - largest - least * (number_of - 1)
    while spare > 0:
        candidates = [i for i in range(1, number_of) if given[i] < largest] or [i for i in range(1, number_of) if given[i] < most]
        mass, budget = sum([weights[i] for i in candidates]), spare
        for i in candidates:
            more = min(most - given[i], max(1, budget * weights[i] // mass), spare)
            given[i] = given[i] + more
            spare = spare - more
    return np.array(given)


def normal_values(rng, shape, deviation, bound, split=(), kind=jnp.bfloat16):
    level = level_of(rng, shape, split, -0.22, 0.18) if split else 1.0
    array = jax.random.normal(rng, shape, jnp.float32) * deviation * level
    return jnp.minimum(jnp.maximum(array, -bound), bound).astype(kind)


def setup_inputs(seed: int = 0) -> dict:
    streams_of = jax.random.split(jax.random.key(seed), 21)
    tokens = normal_values(streams_of[0], (ROWS, D), 1.0, 6.0, ((0, 8), (1, 4)))
    gain_mix = jnp.clip(1.0 + 0.18 * jax.random.normal(streams_of[1], (D,), jnp.float32), 0.1, 1.9)
    w_in = normal_values(streams_of[2], (D, SSM_WIDTH), D ** -0.5, 0.125, ((1, 4),))
    decay_rate = jnp.clip(jnp.exp(math.log(3.0) - 4.0943445 * jax.random.uniform(streams_of[3], (GROUPS, STATE), jnp.float32) ** level_of(streams_of[3], (GROUPS, STATE), ((0, 4),), -0.2, 0.2)), 0.05, 3.0)
    frequency = jnp.clip(jax.random.uniform(streams_of[4], (GROUPS, STATE), jnp.float32, -3.0, 3.0) * level_of(streams_of[4], (GROUPS, STATE), ((0, 4),), -0.4, 0.0), -3.0, 3.0)
    log_step = jnp.clip(-3.0 + 3.0 * jax.random.uniform(streams_of[5], (GROUPS,), jnp.float32) ** level_of(streams_of[5], (GROUPS,), ((0, 4),), -0.2, 0.2), -3.0, 0.0)
    input_real = normal_values(streams_of[6], (GROUPS, STATE, CHANNELS), (2 * CHANNELS) ** -0.5, 1.0, ((0, 4),), jnp.float32)
    input_imag = normal_values(streams_of[7], (GROUPS, STATE, CHANNELS), (2 * CHANNELS) ** -0.5, 1.0, ((0, 4),), jnp.float32)
    readout_real = normal_values(streams_of[8], (GROUPS, CHANNELS, STATE), STATE ** -0.5, 0.75, ((0, 4),), jnp.float32)
    readout_imaginary = normal_values(streams_of[9], (GROUPS, CHANNELS, STATE), STATE ** -0.5, 0.75, ((0, 4),), jnp.float32)
    passthrough_scale = normal_values(streams_of[10], (SSM_WIDTH,), 1.0, 4.0, ((0, 4),), jnp.float32)
    state_real = normal_values(streams_of[11], (ROWS, GROUPS, STATE), 0.5, 4.0, ((0, 8), (1, 4)), jnp.float32)
    state_imag = normal_values(streams_of[12], (ROWS, GROUPS, STATE), 0.5, 4.0, ((0, 8), (1, 4)), jnp.float32)
    w_out = normal_values(streams_of[13], (SSM_WIDTH, D), SSM_WIDTH ** -0.5, 0.1875)
    gain_ffn = jnp.clip(1.0 + 0.18 * jax.random.normal(streams_of[14], (D,), jnp.float32), 0.1, 1.9)
    expert_choice_keys = jax.random.split(jax.random.fold_in(streams_of[15], 1), ROWS // SEQS)
    expert_choice_turns = jax.random.permutation(jax.random.fold_in(streams_of[15], 3), ROWS // SEQS)
    expert_choice = jax.vmap(lambda own, number: shared_out(jax.random.fold_in(streams_of[15], 2), own, number, SEQS, EXPERTS, TOP, CAP, 2))(expert_choice_keys, expert_choice_turns).reshape((ROWS, TOP))
    expert_weight = jnp.clip(0.2 + 0.8 * jax.random.uniform(streams_of[16], (ROWS, TOP), jnp.float32) ** level_of(streams_of[16], (ROWS, TOP), ((0, 8),), -0.2, 0.2), 0.2, 1.0)
    w_gate = normal_values(streams_of[17], (EXPERTS, D, FF), D ** -0.5, 0.125, ((0, 8), (2, 4)))
    w_up = normal_values(streams_of[18], (EXPERTS, D, FF), D ** -0.5, 0.125, ((0, 8), (2, 4)))
    w_down = normal_values(streams_of[19], (EXPERTS, FF, D), FF ** -0.5, 0.0625, ((0, 8), (1, 4)))
    return dict(tokens=tokens, gain_mix=gain_mix, w_in=w_in, decay_rate=decay_rate, frequency=frequency, log_step=log_step, input_real=input_real, input_imag=input_imag, readout_real=readout_real, readout_imaginary=readout_imaginary, passthrough_scale=passthrough_scale, state_real=state_real, state_imag=state_imag, w_out=w_out, gain_ffn=gain_ffn, expert_choice=expert_choice, expert_weight=expert_weight, w_gate=w_gate, w_up=w_up, w_down=w_down)


def rms_norm(values, gains):
    float_values = values.astype(jnp.float32)
    scale = lax.rsqrt(lax.optimization_barrier(jnp.mean(float_values * float_values, axis=-1, keepdims=True)) + 1e-06)
    return (float_values * scale * gains).astype(jnp.bfloat16)

def state_step(drive, real_state, imag_state, decay_rate, frequency, log_step, input_real, input_imag, readout_real, readout_imaginary, passthrough_scale):
    highest_precision = lax.Precision.HIGHEST
    count_of_groups, count_of_channels = (input_real.shape[0], input_real.shape[2])
    step = jnp.exp(log_step)[:, None]
    lam_real = -decay_rate
    magnitude = jnp.exp(lam_real * step)
    abar_real = magnitude * jnp.cos(frequency * step)
    abar_imag = magnitude * jnp.sin(frequency * step)
    denom = lam_real * lam_real + frequency * frequency
    numer = abar_real - 1.0
    factor_real = (numer * lam_real + abar_imag * frequency) / denom
    factor_imag = (abar_imag * lam_real - numer * frequency) / denom
    bbar_real = factor_real[..., None] * input_real - factor_imag[..., None] * input_imag
    bbar_imag = factor_real[..., None] * input_imag + factor_imag[..., None] * input_real
    float_values = drive.astype(jnp.float32).reshape(drive.shape[0], count_of_groups, count_of_channels)
    push_real = jnp.einsum('sgc,gpc->sgp', float_values, bbar_real, precision=highest_precision)
    push_imag = jnp.einsum('sgc,gpc->sgp', float_values, bbar_imag, precision=highest_precision)
    next_state_real = abar_real * real_state - abar_imag * imag_state + push_real
    next_state_imaginary = abar_real * imag_state + abar_imag * real_state + push_imag
    readout_matrix = jnp.einsum('jdr,dyr->jdy', next_state_real, readout_real, precision=highest_precision) - jnp.einsum('jdr,dyr->jdy', next_state_imaginary, readout_imaginary, precision=highest_precision) + passthrough_scale.reshape(count_of_groups, count_of_channels) * float_values
    mixer = jax.nn.gelu(readout_matrix.reshape(drive.shape[0], count_of_groups * count_of_channels)).astype(jnp.bfloat16)
    return (mixer, next_state_real, next_state_imaginary)

def slot_table(routes, expert_count, capacity):
    flat = routes.reshape(-1)
    onehot = (flat[:, None] == jnp.arange(expert_count, dtype=jnp.int32)[None, :]).astype(jnp.int32)
    before = jnp.cumsum(onehot, axis=0) - onehot
    slot = lax.optimization_barrier(jnp.sum(before * onehot, axis=1))
    target = flat * capacity + slot
    return (target[None, :] == jnp.arange(expert_count * capacity, dtype=jnp.int32)[:, None]).astype(jnp.bfloat16)

def reference(tokens, gain_mix, w_in, decay_rate, frequency, log_step, input_real, input_imag, readout_real, readout_imaginary, passthrough_scale, state_real, state_imag, w_out, gain_ffn, expert_choice, expert_weight, w_gate, w_up, w_down):
    normed = rms_norm(tokens, gain_mix)
    drive = jnp.dot(normed, w_in, preferred_element_type=jnp.float32).astype(jnp.bfloat16)
    mixer, next_state_real, next_state_imaginary = state_step(drive, state_real, state_imag, decay_rate, frequency, log_step, input_real, input_imag, readout_real, readout_imaginary, passthrough_scale)
    mixed = jnp.dot(mixer, w_out, preferred_element_type=jnp.float32).astype(jnp.bfloat16)
    after_mix = (tokens.astype(jnp.float32) + mixed.astype(jnp.float32)).astype(jnp.bfloat16)
    normed_ffn = rms_norm(after_mix, gain_ffn)
    group_rows = normed_ffn.reshape(N_EP, SEQS, D)
    routes = expert_choice.reshape(N_EP, SEQS, TOP)
    tables = jax.vmap(lambda block: slot_table(block, EXPERTS, CAP))(routes).astype(jnp.float32)
    repeated = jnp.repeat(group_rows, TOP, axis=1).astype(jnp.float32)
    sent = jnp.einsum('gks,gsd->gkd', tables, repeated).astype(jnp.bfloat16)
    sent = jnp.moveaxis(sent.reshape(N_EP, EXPERTS, CAP, D), 1, 0)
    slice_width = FF // N_TP

    def expert(inputs):
        arrived, gate_w, up_w, down_w = inputs
        flat = arrived.reshape(N_EP * CAP, D)
        gate = jnp.dot(flat, gate_w, preferred_element_type=jnp.float32)
        upper = jnp.dot(flat, up_w, preferred_element_type=jnp.float32)
        hidden = (jax.nn.silu(gate) * upper).astype(jnp.bfloat16)
        pieces = hidden.reshape(N_EP * CAP, N_TP, slice_width).astype(jnp.float32)
        downs = down_w.reshape(N_TP, slice_width, D).astype(jnp.float32)
        partial_value = jnp.einsum('rtf,tfd->rtd', pieces, downs).astype(jnp.bfloat16)
        partial_value = lax.optimization_barrier(partial_value)
        return lax.optimization_barrier(jnp.sum(partial_value.astype(jnp.float32), axis=1)).astype(jnp.bfloat16)
    results = lax.map(expert, (sent, w_gate, w_up, w_down))
    results = jnp.moveaxis(results.reshape(EXPERTS, N_EP, CAP, D), 1, 0).reshape(N_EP, EXPERTS * CAP, D)
    picked = jnp.einsum('gks,gkd->gsd', tables, results.astype(jnp.float32)).reshape(N_EP, SEQS, TOP, D)
    weighted = lax.optimization_barrier(jnp.sum(picked * expert_weight.reshape(N_EP, SEQS, TOP)[..., None], axis=2)).reshape(ROWS, D)
    layer_out = (after_mix.astype(jnp.float32) + weighted).astype(jnp.bfloat16)
    return (layer_out, next_state_real, next_state_imaginary)
```

```python
import functools
from types import SimpleNamespace

import jax
import jax.numpy as jnp
from jax import lax
from jax.experimental import pallas as pl
from jax.experimental.pallas import tpu as pltpu
from jax.sharding import PartitionSpec as P


def state_step(
    drive,
    real_state,
    imag_state,
    decay_rate,
    frequency,
    log_step,
    input_real,
    input_imag,
    readout_real,
    readout_imaginary,
    passthrough_scale,
):
    highest_precision = lax.Precision.HIGHEST
    count_of_groups, count_of_channels = (input_real.shape[0], input_real.shape[2])
    step = jnp.exp(log_step)[:, None]
    lam_real = -decay_rate
    magnitude = jnp.exp(lam_real * step)
    abar_real = magnitude * jnp.cos(frequency * step)
    abar_imag = magnitude * jnp.sin(frequency * step)
    denom = lam_real * lam_real + frequency * frequency
    numer = abar_real - 1.0
    factor_real = (numer * lam_real + abar_imag * frequency) / denom
    factor_imag = (abar_imag * lam_real - numer * frequency) / denom
    bbar_real = factor_real[..., None] * input_real - factor_imag[..., None] * input_imag
    bbar_imag = factor_real[..., None] * input_imag + factor_imag[..., None] * input_real
    float_values = drive.astype(jnp.float32).reshape(
        drive.shape[0], count_of_groups, count_of_channels
    )
    push_real = jnp.einsum("sgc,gpc->sgp", float_values, bbar_real, precision=highest_precision)
    push_imag = jnp.einsum("sgc,gpc->sgp", float_values, bbar_imag, precision=highest_precision)
    next_state_real = abar_real * real_state - abar_imag * imag_state + push_real
    next_state_imaginary = abar_real * imag_state + abar_imag * real_state + push_imag
    readout_matrix = (
        jnp.einsum("jdr,dyr->jdy", next_state_real, readout_real, precision=highest_precision)
        - jnp.einsum(
            "jdr,dyr->jdy", next_state_imaginary, readout_imaginary, precision=highest_precision
        )
        + passthrough_scale.reshape(count_of_groups, count_of_channels) * float_values
    )
    mixer = jax.nn.gelu(
        readout_matrix.reshape(drive.shape[0], count_of_groups * count_of_channels)
    ).astype(jnp.bfloat16)
    return (mixer, next_state_real, next_state_imaginary)


def slot_table(routes, expert_count, capacity):
    flat = routes.reshape(-1)
    onehot = (flat[:, None] == jnp.arange(expert_count, dtype=jnp.int32)[None, :]).astype(jnp.int32)
    before = jnp.cumsum(onehot, axis=0) - onehot
    slot = jnp.sum(before * onehot, axis=1)
    target = flat * capacity + slot
    return (
        target[None, :] == jnp.arange(expert_count * capacity, dtype=jnp.int32)[:, None]
    ).astype(jnp.bfloat16)


def flipped(index, mask, count):
    other = 0
    bit = 1
    while bit < count:
        digit = lax.rem(lax.div(index, bit), 2)
        other = other + bit * ((1 - digit) if mask & bit else digit)
        bit *= 2
    return other


def dot(left, right):
    return jnp.dot(left, right, preferred_element_type=jnp.float32)


def halves(values):
    high = values.astype(jnp.bfloat16)
    return high, (values - high.astype(jnp.float32)).astype(jnp.bfloat16)


def layer_kernel(ep_count, tp_count, sizes, *refs):
    names_in, names_out, names_scratch = sizes
    r = SimpleNamespace(**dict(zip(names_in + names_out + names_scratch, refs)))
    me_ep, me_tp = lax.axis_index("ep"), lax.axis_index("tp")
    capacity, width = r.out_tok.shape[1], r.out_tok.shape[2]
    channels = r.out_mix.shape[2]
    pairs = ep_count // 2
    slots = ep_count * capacity
    full = width * tp_count
    row_count = r.pieces.shape[1]
    f32, bf16 = jnp.float32, jnp.bfloat16
    tp_of = [flipped(me_tp, p, tp_count) for p in range(tp_count)]
    ep_of = [flipped(me_ep, j, ep_count) for j in range(ep_count)]

    barrier = pltpu.get_barrier_semaphore()
    for p in range(1, tp_count):
        pl.semaphore_signal(
            barrier, inc=1, device_id={"tp": tp_of[p]}, device_id_type=pl.DeviceIdType.MESH
        )
    for j in range(1, ep_count):
        pl.semaphore_signal(
            barrier, inc=1, device_id={"ep": ep_of[j]}, device_id_type=pl.DeviceIdType.MESH
        )

    loads = []

    def load(source, target):
        loads.append(pltpu.make_async_copy(source, target, r.load_sem.at[len(loads)]))
        loads[-1].start()
        return loads[-1]

    load_tokens = load(r.tokens, r.pieces.at[0])
    load_routes = [load(r.choice, r.choice_v), load(r.weight, r.weight_v)]
    load_small = [
        load(r.decay, r.decay_v),
        load(r.freq, r.freq_v),
        load(r.step, r.step_v),
        load(r.pass_, r.pass_v),
        load(r.gain_mix, r.gain_mix_v),
        load(r.gain_ffn, r.gain_ffn_v),
    ]
    load_mats = [
        load(r.in_re, r.in_re_v),
        load(r.in_im, r.in_im_v),
        load(r.re_re, r.re_re_v),
        load(r.re_im, r.re_im_v),
    ]
    load_w_in = load(r.w_in, r.w_in_v)
    load_states = [load(r.state_r, r.state_rv), load(r.state_i, r.state_iv)]
    load_w_out = load(r.w_out, r.w_out_v)
    load_gates = [load(r.gate.at[0], r.gate_v), load(r.up.at[0], r.up_v)]
    load_down = load(r.down.at[0], r.down_v)

    def remote(src, dst, send, recv, **where):
        return pltpu.make_async_remote_copy(
            src_ref=src,
            dst_ref=dst,
            send_sem=send,
            recv_sem=recv,
            device_id=where,
            device_id_type=pl.DeviceIdType.MESH,
        )

    started = []

    def go(copy):
        copy.start()
        started.append(copy)
        return copy

    load_tokens.wait()
    pl.semaphore_wait(barrier, tp_count - 1 + ep_count - 1)
    first = {
        p: go(remote(r.pieces.at[0], r.pieces.at[p], r.a_send.at[p], r.a_recv.at[p],
                     tp=tp_of[p]))
        for p in (3, 1, 2)
    }

    for copy in load_routes:
        copy.wait()
    choice, weight = r.choice_v[...], r.weight_v[...]
    top_count = choice.shape[0]
    experts = lax.broadcasted_iota(jnp.int32, (ep_count, row_count), 0)
    picks = [(choice[k : k + 1] == experts).astype(f32) for k in range(top_count)]
    earlier = (
        lax.broadcasted_iota(jnp.int32, (row_count, row_count), 0)
        < lax.broadcasted_iota(jnp.int32, (row_count, row_count), 1)
    ).astype(bf16)
    before = dot(sum(picks).astype(bf16), earlier)
    spots = lax.broadcasted_iota(jnp.int32, (slots, row_count), 0)
    table, weights = 0.0, 0.0
    for k in range(top_count):
        slot = jnp.sum(before * picks[k], axis=0, keepdims=True).astype(jnp.int32)
        hit = (choice[k : k + 1] * capacity + slot == spots).astype(f32)
        table = table + hit
        weights = weights + hit * weight[k : k + 1]
        before = before + picks[k]
    table = table.astype(bf16)
    r.table[...] = table.reshape(ep_count, capacity, row_count)
    r.out_tok[...] = dot(table, r.pieces[0]).astype(bf16).reshape(ep_count, capacity, width)

    def spread(source, arrived, send, recv):
        copies = {}
        for j in range(2, ep_count):
            copies[j] = go(remote(source.at[ep_of[j]], arrived.at[0, j], send.at[j], recv.at[j],
                                  ep=ep_of[j]))
        return copies

    tok_z = spread(r.out_tok, r.arr_tok, r.bz_send, r.bz_recv)
    tok_near, tok_far, mix_near, mix_far = {}, {}, {}, {}

    def forward(m, peers, z_copies, arrived, near, send, recv):
        for j in (2 * m, 2 * m + 1):
            z_copies[j].wait_recv()
        block = pl.ds(2 * m, 2)
        for p in peers:
            near[p, m] = go(remote(arrived.at[0, block], arrived.at[p, block], send.at[p, m],
                                   recv.at[p, m], tp=tp_of[p]))

    def tok_forward(m):
        forward(m, (1, 2), tok_z, r.arr_tok, tok_near, r.bn_send, r.bn_recv)

    def tok_relay(m):
        for p in (1, 2):
            tok_near[p, m].wait_recv()
            j = 2 * m + p - 1
            tok_far[p, m] = go(remote(r.arr_tok.at[p, j], r.arr_tok.at[3, j], r.bf_send.at[p, m],
                                      r.bf_recv.at[p, m], tp=tp_of[3 - p]))

    def share(pieces, shared, arrived, send, recv):
        for p in range(tp_count):
            piece = pieces[p]
            arrived[p, 0] = dot(r.table[me_ep], piece).astype(bf16)
            shared[p] = dot(r.table[ep_of[1]], piece).astype(bf16)
        return [
            go(remote(shared.at[p], arrived.at[p, 1], send.at[p], recv.at[p], ep=ep_of[1]))
            for p in range(tp_count)
        ]

    groups = r.decay.shape[0]
    entries = r.in_re_v.shape[1]
    per_group = channels // groups
    eye = (
        lax.broadcasted_iota(jnp.int32, (groups, groups), 0)
        == lax.broadcasted_iota(jnp.int32, (groups, groups), 1)
    ).astype(f32)
    for copy in load_small:
        copy.wait()
    step = jnp.sum(eye * jnp.exp(r.step_v[...]), axis=1, keepdims=True)
    lam = -r.decay_v[...]
    frequency = r.freq_v[...]
    magnitude = jnp.exp(lam * step)
    abar_real = magnitude * jnp.cos(frequency * step)
    abar_imag = magnitude * jnp.sin(frequency * step)
    denom = lam * lam + frequency * frequency
    numer = abar_real - 1.0
    factor_real = (numer * lam + abar_imag * frequency) / denom
    factor_imag = (abar_imag * lam - numer * frequency) / denom

    def per_channel(values):
        return jnp.broadcast_to(values[:, None, :], (groups, per_group, entries)).reshape(
            channels, entries
        )

    wide_real, wide_imag = per_channel(factor_real), per_channel(factor_imag)
    for copy in load_mats:
        copy.wait()
    in_re, in_im = r.in_re_v[...], r.in_im_v[...]
    push_w = jnp.concatenate(
        [wide_real * in_re - wide_imag * in_im, wide_real * in_im + wide_imag * in_re], axis=1
    )
    push_high, push_low = halves(push_w)
    r.push_w[0], r.push_w[1] = push_high, push_low
    read_w = jnp.concatenate([r.re_re_v[...], -r.re_im_v[...]], axis=1).T
    read_high, read_low = halves(read_w)
    r.read_w[0], r.read_w[1] = read_high, read_low
    weight_high, weight_low = halves(weights.T)
    r.combine[0], r.combine[1] = weight_high, weight_low
    rows = row_count * groups
    r.replicate[...] = (
        lax.broadcasted_iota(jnp.int32, (rows, row_count), 0) // groups
        == lax.broadcasted_iota(jnp.int32, (rows, row_count), 1)
    ).astype(bf16)
    r.own_group[...] = (
        lax.broadcasted_iota(jnp.int32, (groups, channels), 0)
        == lax.broadcasted_iota(jnp.int32, (groups, channels), 1) // per_group
    ).astype(f32)
    r.abar[0], r.abar[1] = abar_real, abar_imag

    early, middle, late = (range(1, pairs)[part] for part in (slice(1), slice(1, 2), slice(2, None)))
    for m in early:
        tok_forward(m)

    squares, drive = 0.0, None
    for p in (0, 1, 2, 3):
        if p:
            first[p].wait_recv()
        piece = r.pieces[p].astype(f32)
        squares = squares + jnp.sum(piece * piece, axis=1, keepdims=True)
        if not p:
            load_w_in.wait()
        term = dot((piece * r.gain_mix_v[tp_of[p]]).astype(bf16), r.w_in_v[tp_of[p]])
        drive = term if drive is None else drive + term
    drive = (drive * lax.rsqrt(squares / full + 1e-06)).astype(bf16)

    for m in middle:
        tok_forward(m)
    spread_drive = dot(r.replicate[...], drive).reshape(row_count, groups, channels)
    spread_drive = (spread_drive * r.own_group[...]).astype(bf16).reshape(rows, channels)
    push = dot(spread_drive, r.push_w[0]) + dot(spread_drive, r.push_w[1])
    for copy in load_states:
        copy.wait()

    def per_row(values):
        return jnp.broadcast_to(values[None], (row_count, groups, entries)).reshape(rows, entries)

    wide_real, wide_imag = per_row(r.abar[0]), per_row(r.abar[1])
    real, imag = r.state_rv[...], r.state_iv[...]
    next_real = wide_real * real - wide_imag * imag + push[:, :entries]
    next_imag = wide_real * imag + wide_imag * real + push[:, entries:]
    r.next_r[...] = next_real
    r.next_i[...] = next_imag
    for m in late:
        tok_forward(m)
    both_high, both_low = halves(jnp.concatenate([next_real, next_imag], axis=1))
    spread_y = (
        dot(both_high, r.read_w[0])
        + dot(both_low, r.read_w[0])
        + dot(both_high, r.read_w[1])
    )
    lane_group = lax.broadcasted_iota(jnp.int32, (row_count, 128), 1) // per_group
    lane_groups = 128 // per_group
    readout = []
    for t in range(channels // 128):
        r.spread_y[t] = spread_y[:, t * 128 : (t + 1) * 128]
        picked = None
        for g in range(lane_groups):
            strip = r.spread_y[t, pl.ds(t * lane_groups + g, row_count, groups), :]
            picked = strip if picked is None else jnp.where(lane_group == g, strip, picked)
        readout.append(picked)
    readout = jnp.concatenate(readout, axis=1) + r.pass_v[...] * drive.astype(f32)
    mixer = jax.nn.gelu(readout).astype(bf16)
    r.mixers[0] = mixer

    own_mix = {
        p: go(remote(r.mixers.at[0], r.mixers.at[p], r.e_send.at[p], r.e_recv.at[p], tp=tp_of[p]))
        for p in (3, 1, 2)
    }
    r.out_mix[...] = dot(table, mixer).astype(bf16).reshape(ep_count, capacity, channels)
    mix_z = spread(r.out_mix, r.arr_mix, r.cz_send, r.cz_recv)

    def mix_forward(m):
        forward(m, (3, 1, 2), mix_z, r.arr_mix, mix_near, r.cn_send, r.cn_recv)

    tok_share = share(r.pieces, r.shared_tok, r.arr_tok, r.bs_send, r.bs_recv)
    for m in range(1, pairs):
        tok_relay(m)
        mix_forward(m)
    for p in (1, 2, 3):
        own_mix[p].wait_recv()
    mix_share = share(r.mixers, r.shared_mix, r.arr_mix, r.cs_send, r.cs_recv)
    for copy in mix_share:
        copy.wait_recv()
    load_w_out.wait()
    mixed = r.mixed
    for p in (0, 1, 2):
        if p:
            for m in range(1, pairs):
                mix_near[p, m].wait_recv()
        block = r.arr_mix[p].reshape(slots, channels)
        for n in range(tp_count):
            columns = pl.ds(n * width, width)
            term = dot(block, r.w_out_v[tp_of[p], :, columns])
            mixed[:, columns] = term if p == 0 else mixed[:, columns] + term
    for copy in tok_share:
        copy.wait_recv()
    for m in range(1, pairs):
        mix_near[3, m].wait_recv()
        for p in (1, 2):
            tok_far[p, m].wait_recv()
    block = r.arr_mix[3].reshape(slots, channels)
    squares = 0.0
    for n in range(tp_count):
        columns = pl.ds(n * width, width)
        term = mixed[:, columns] + dot(block, r.w_out_v[tp_of[3], :, columns])
        after = r.arr_tok[tp_of[n]].reshape(slots, width).astype(f32)
        after = (after + term.astype(bf16).astype(f32)).astype(bf16).astype(f32)
        squares = squares + jnp.sum(after * after, axis=1, keepdims=True)
        r.normed[:, columns] = (after * r.gain_ffn_v[n]).astype(bf16)
    scale = lax.rsqrt(squares / full + 1e-06)

    r.scale[...] = jnp.broadcast_to(scale, r.scale.shape)
    for copy in load_gates:
        copy.wait()
    load_down.wait()
    hidden_width = r.hidden.shape[1]
    tile = next(t for t in (512, 256, 128) if hidden_width % t == 0)
    half = slots // 2

    def gate_up(first):
        span = pl.ds(first, half)

        @pl.loop(0, hidden_width // tile)
        def _(n):
            columns = pl.ds(pl.multiple_of(n * tile, tile), tile)
            scale = r.scale[span, :1]
            gate = dot(r.normed[span], r.gate_v[:, columns]) * scale
            upper = dot(r.normed[span], r.up_v[:, columns]) * scale
            r.hidden[span, columns] = (jax.nn.silu(gate) * upper).astype(bf16)

    def rows_of(j):
        return pl.ds(j * capacity, capacity)

    parts, relay_in, parts_in, held = r.parts, r.relay_in, r.parts_in, r.held
    far_send, pure_send, merged_send = {}, {}, {}

    def down(p, first):
        columns = pl.ds(pl.multiple_of(tp_of[p] * width, width), width)
        return dot(r.hidden[pl.ds(first, half)], r.down_v[:, columns])

    def down_far(first, chunk):
        parts[3, pl.ds(first, half)] = down(3, first).astype(bf16)
        for m in chunk:
            for p in (1, 2):
                j = 2 * m + p - 1
                far_send[p, m] = go(remote(parts.at[3, rows_of(j)], relay_in.at[rows_of(j)],
                                           r.rf_send.at[p, m], r.rf_recv.at[p, m], tp=tp_of[p]))

    def down_near(first, chunk):
        for p in (1, 2):
            value = down(p, first)
            held[p, pl.ds(first, half)] = value
            parts[p, pl.ds(first, half)] = value.astype(bf16)
            for m in chunk:
                j = 2 * m + p - 1
                pure_send[p, m] = go(remote(parts.at[p, rows_of(j)], parts_in.at[p, rows_of(j)],
                                            r.rp_send.at[p, m], r.rp_recv.at[p, m], tp=tp_of[p]))

    def down_own(first):
        held[0, pl.ds(first, half)] = down(0, first)

    def merge(m):
        for p in (1, 2):
            q = 3 - p
            j = 2 * m + p - 1
            far_send[p, m].wait_recv()
            merged = held[q, rows_of(j)] + relay_in[rows_of(j)].astype(f32)
            r.merged[rows_of(j)] = merged.astype(bf16)
            merged_send[q, m] = go(remote(r.merged.at[rows_of(j)], parts_in.at[q, rows_of(j)],
                                          r.rm_send.at[q, m], r.rm_recv.at[q, m], tp=tp_of[q]))

    back = {}

    def finish(m):
        for p in (1, 2):
            pure_send[p, m].wait_recv()
            merged_send[p, m].wait_recv()
        span = pl.ds(2 * m * capacity, 2 * capacity)
        total = held[0, span] + parts_in[1, span].astype(f32) + parts_in[2, span].astype(f32)
        r.results[pl.ds(2 * m, 2)] = total.astype(bf16).reshape(2, capacity, width)
        for j in (2 * m + 1, 2 * m):
            if j:
                back[j] = go(remote(r.results.at[j], r.returned.at[me_ep],
                                    r.z_send.at[j], r.z_recv.at[j], ep=ep_of[j]))

    far_half = tuple(reversed(range(pairs // 2, pairs)))
    near_half = tuple(reversed(range(pairs // 2)))
    gate_up(half)
    down_far(half, far_half)
    down_near(half, far_half)
    down_own(half)
    gate_up(0)
    for m in far_half:
        merge(m)
    down_far(0, near_half)
    down_near(0, near_half)
    down_own(0)
    for m in far_half:
        finish(m)
    for m in near_half:
        merge(m)
    for m in near_half[:-1]:
        finish(m)
    own = pl.ds(pl.multiple_of(me_tp * width, width), width)
    mixed_own = None
    for p in range(tp_count):
        term = dot(r.mixers[p], r.w_out_v[tp_of[p], :, own])
        mixed_own = term if mixed_own is None else mixed_own + term
    after_own = (
        (r.pieces[0].astype(f32) + mixed_own.astype(bf16).astype(f32)).astype(bf16).astype(f32)
    )
    finish(0)
    r.returned[me_ep] = r.results[0]
    for j in range(1, ep_count):
        remote(r.results.at[j], r.returned.at[ep_of[j]], r.z_send.at[j],
               r.z_recv.at[j], ep=ep_of[j]).wait_recv()
    everything = r.returned[...].reshape(slots, width)
    weighted = dot(r.combine[0], everything) + dot(r.combine[1], everything)
    r.out[...] = (after_own + weighted).astype(bf16)
    for copy in started:
        copy.wait_send()


def layer_call(
    tokens, gain_mix, w_in, decay_rate, frequency, log_step, input_real, input_imag, readout_real,
    readout_imaginary, passthrough_scale, state_real, state_imag, w_out, gain_ffn, expert_choice,
    expert_weight, w_gate, w_up, w_down, capacity, ep_count, tp_count,
):
    row_count, width = tokens.shape
    full = width * tp_count
    groups, entries, per_group = input_real.shape
    channels = groups * per_group
    slots = ep_count * capacity
    pairs = ep_count // 2
    hidden_width = w_gate.shape[2]
    rows = row_count * groups
    bf16, f32 = jnp.bfloat16, jnp.float32
    vmem = pl.BlockSpec(memory_space=pltpu.VMEM)
    hbm = pl.BlockSpec(memory_space=pl.ANY)
    inputs = dict(
        tokens=(tokens, hbm),
        gain_mix=(gain_mix.reshape(tp_count, 1, width), hbm),
        gain_ffn=(gain_ffn.reshape(tp_count, 1, width), hbm),
        decay=(decay_rate, hbm),
        freq=(frequency, hbm),
        step=(log_step.reshape(1, groups), hbm),
        pass_=(passthrough_scale.reshape(1, channels), hbm),
        choice=(expert_choice.T, hbm),
        weight=(expert_weight.T, hbm),
        in_re=(jnp.transpose(input_real, (0, 2, 1)).reshape(channels, entries), hbm),
        in_im=(jnp.transpose(input_imag, (0, 2, 1)).reshape(channels, entries), hbm),
        re_re=(readout_real.reshape(channels, entries), hbm),
        re_im=(readout_imaginary.reshape(channels, entries), hbm),
        state_r=(state_real.reshape(rows, entries), hbm),
        state_i=(state_imag.reshape(rows, entries), hbm),
        w_in=(w_in.reshape(tp_count, width, channels), hbm),
        w_out=(w_out.reshape(tp_count, channels, full), hbm),
        gate=(w_gate, hbm),
        up=(w_up, hbm),
        down=(w_down, hbm),
    )
    outputs = dict(
        out=pltpu.VMEM((row_count, width), bf16),
        next_r=pltpu.VMEM((rows, entries), f32),
        next_i=pltpu.VMEM((rows, entries), f32),
    )
    dma = lambda *shape: pltpu.SemaphoreType.DMA(shape)
    scratch = dict(
        pieces=pltpu.VMEM((tp_count, row_count, width), bf16),
        choice_v=pltpu.VMEM(expert_choice.shape[::-1], expert_choice.dtype),
        weight_v=pltpu.VMEM(expert_weight.shape[::-1], f32),
        decay_v=pltpu.VMEM((groups, entries), f32),
        freq_v=pltpu.VMEM((groups, entries), f32),
        step_v=pltpu.VMEM((1, groups), f32),
        pass_v=pltpu.VMEM((1, channels), f32),
        gain_mix_v=pltpu.VMEM((tp_count, 1, width), f32),
        gain_ffn_v=pltpu.VMEM((tp_count, 1, width), f32),
        table=pltpu.VMEM((ep_count, capacity, row_count), bf16),
        replicate=pltpu.VMEM((rows, row_count), bf16),
        own_group=pltpu.VMEM((groups, channels), f32),
        abar=pltpu.VMEM((2, groups, entries), f32),
        shared_tok=pltpu.VMEM((tp_count, capacity, width), bf16),
        shared_mix=pltpu.VMEM((tp_count, capacity, channels), bf16),
        scale=pltpu.VMEM((slots, 128), f32),
        in_re_v=pltpu.VMEM((channels, entries), f32),
        in_im_v=pltpu.VMEM((channels, entries), f32),
        re_re_v=pltpu.VMEM((channels, entries), f32),
        re_im_v=pltpu.VMEM((channels, entries), f32),
        state_rv=pltpu.VMEM((rows, entries), f32),
        state_iv=pltpu.VMEM((rows, entries), f32),
        w_in_v=pltpu.VMEM((tp_count, width, channels), bf16),
        w_out_v=pltpu.VMEM((tp_count, channels, full), bf16),
        gate_v=pltpu.VMEM((full, hidden_width), bf16),
        up_v=pltpu.VMEM((full, hidden_width), bf16),
        down_v=pltpu.VMEM((hidden_width, full), bf16),
        push_w=pltpu.VMEM((2, channels, 2 * entries), bf16),
        read_w=pltpu.VMEM((2, 2 * entries, channels), bf16),
        combine=pltpu.VMEM((2, row_count, slots), bf16),
        spread_y=pltpu.VMEM((channels // 128, rows, 128), f32),
        mixers=pltpu.VMEM((tp_count, row_count, channels), bf16),
        out_tok=pltpu.VMEM((ep_count, capacity, width), bf16),
        arr_tok=pltpu.VMEM((tp_count, ep_count, capacity, width), bf16),
        out_mix=pltpu.VMEM((ep_count, capacity, channels), bf16),
        arr_mix=pltpu.VMEM((tp_count, ep_count, capacity, channels), bf16),
        mixed=pltpu.VMEM((slots, full), f32),
        normed=pltpu.VMEM((slots, full), bf16),
        hidden=pltpu.VMEM((slots, hidden_width), bf16),
        parts=pltpu.VMEM((tp_count, slots, width), bf16),
        held=pltpu.VMEM((3, slots, width), f32),
        relay_in=pltpu.VMEM((slots, width), bf16),
        merged=pltpu.VMEM((slots, width), bf16),
        parts_in=pltpu.VMEM((3, slots, width), bf16),
        results=pltpu.VMEM((ep_count, capacity, width), bf16),
        returned=pltpu.VMEM((ep_count, capacity, width), bf16),
        load_sem=dma(20),
    )
    kinds = dict(
        a=(tp_count,), e=(tp_count,), bs=(tp_count,), cs=(tp_count,), bz=(ep_count,), cz=(ep_count,), z=(ep_count,),
        bn=(3, pairs), bf=(3, pairs), cn=(4, pairs),
        rf=(3, pairs), rp=(3, pairs), rm=(3, pairs),
    )
    for name, shape in kinds.items():
        scratch[name + "_send"], scratch[name + "_recv"] = dma(*shape), dma(*shape)
    names = (tuple(inputs), tuple(outputs), tuple(scratch))
    out, next_real, next_imag = pl.pallas_call(
        functools.partial(layer_kernel, ep_count, tp_count, names),
        out_shape=tuple(outputs.values()),
        in_specs=[spec for _, spec in inputs.values()],
        out_specs=(vmem, vmem, vmem),
        scratch_shapes=list(scratch.values()),
        compiler_params=pltpu.CompilerParams(
            collective_id=0, has_side_effects=True, vmem_limit_bytes=60 * 1024 * 1024
        ),
    )(*[value for value, _ in inputs.values()])
    shape = (row_count, groups, entries)
    return out, next_real.reshape(shape), next_imag.reshape(shape)


def plain_experts(normed, after, table, expert_weight, w_gate, w_up, w_down):
    row_count, top_count = expert_weight.shape
    expert_count = lax.axis_size("ep")
    capacity = table.shape[0] // expert_count
    width = normed.shape[1]
    repeated = jnp.repeat(normed, top_count, axis=0)
    sent = jnp.dot(table, repeated, preferred_element_type=jnp.float32).astype(jnp.bfloat16)
    sent = sent.reshape(expert_count, capacity, width)
    arrived = lax.all_to_all(sent, "ep", split_axis=0, concat_axis=0, tiled=True)
    flat = arrived.reshape(expert_count * capacity, width)
    piece = lax.all_gather(flat, "tp", axis=1, tiled=True)
    gate = jnp.dot(piece, w_gate[0], preferred_element_type=jnp.float32)
    upper = jnp.dot(piece, w_up[0], preferred_element_type=jnp.float32)
    hidden = (jax.nn.silu(gate) * upper).astype(jnp.bfloat16)
    partial_value = jnp.dot(hidden, w_down[0], preferred_element_type=jnp.float32)
    summed = lax.psum_scatter(
        partial_value.astype(jnp.bfloat16), "tp", scatter_dimension=1, tiled=True
    )
    results = summed.reshape(expert_count, capacity, width)
    returned = lax.all_to_all(results, "ep", split_axis=0, concat_axis=0, tiled=True)
    returned = returned.reshape(expert_count * capacity, width)
    picked = jnp.dot(table.T, returned, preferred_element_type=jnp.float32)
    picked = picked.reshape(row_count, top_count, width)
    weighted = jnp.sum(picked * expert_weight[..., None], axis=1)
    return (after.astype(jnp.float32) + weighted).astype(jnp.bfloat16)


def norm(values, gains):
    floats = values.astype(jnp.float32)
    scale = lax.rsqrt(jnp.mean(floats * floats, axis=1, keepdims=True) + 1e-06)
    return (floats * scale * gains).astype(jnp.bfloat16)


def power_of_two(count):
    return count & (count - 1) == 0


def body(
    tokens,
    gain_mix,
    w_in,
    decay_rate,
    frequency,
    log_step,
    input_real,
    input_imag,
    readout_real,
    readout_imaginary,
    passthrough_scale,
    state_real,
    state_imag,
    w_out,
    gain_ffn,
    expert_choice,
    expert_weight,
    w_gate,
    w_up,
    w_down,
):
    tp_count = lax.axis_size("tp")
    expert_count = lax.axis_size("ep")
    row_count, local_width = tokens.shape
    feature_start = lax.axis_index("tp") * local_width
    top_count = expert_choice.shape[1]
    capacity = 2 * row_count * top_count // expert_count
    fused = (
        local_width % 128 == 0
        and w_gate.shape[2] % 128 == 0
        and capacity % 16 == 0
        and tp_count == 4
        and power_of_two(expert_count)
        and 4 <= expert_count <= 8
        and w_in.shape[1] % 128 == 0
        and row_count % 16 == 0
        and input_real.shape[0] % 8 == 0
        and input_real.shape[1] == 64
        and 128 % input_real.shape[2] == 0
    )
    if fused:
        return layer_call(
            tokens,
            gain_mix,
            w_in,
            decay_rate,
            frequency,
            log_step,
            input_real,
            input_imag,
            readout_real,
            readout_imaginary,
            passthrough_scale,
            state_real,
            state_imag,
            w_out,
            gain_ffn,
            expert_choice,
            expert_weight,
            w_gate,
            w_up,
            w_down,
            capacity,
            expert_count,
            tp_count,
        )
    all_tokens = lax.all_gather(tokens, "tp", axis=1, tiled=True)
    drive = jnp.dot(
        norm(all_tokens, gain_mix), w_in, preferred_element_type=jnp.float32
    ).astype(jnp.bfloat16)
    mixer, next_state_real, next_state_imaginary = state_step(
        drive,
        state_real,
        state_imag,
        decay_rate,
        frequency,
        log_step,
        input_real,
        input_imag,
        readout_real,
        readout_imaginary,
        passthrough_scale,
    )
    table = slot_table(expert_choice, expert_count, capacity)
    mixed = jnp.dot(
        lax.all_gather(mixer, "tp", axis=1, tiled=True), w_out, preferred_element_type=jnp.float32
    ).astype(jnp.bfloat16)
    after_all = (all_tokens.astype(jnp.float32) + mixed.astype(jnp.float32)).astype(jnp.bfloat16)
    normed_all = norm(after_all, gain_ffn)
    after = lax.dynamic_slice_in_dim(after_all, feature_start, local_width, 1)
    normed = lax.dynamic_slice_in_dim(normed_all, feature_start, local_width, 1)
    layer_out = plain_experts(normed, after, table, expert_weight, w_gate, w_up, w_down)
    return (layer_out, next_state_real, next_state_imaginary)


def solution(mesh):
    return jax.shard_map(
        body,
        mesh=mesh,
        in_specs=(
            P("ep", "tp"),
            P(),
            P(None, "tp"),
            P("tp", None),
            P("tp", None),
            P("tp"),
            P("tp", None, None),
            P("tp", None, None),
            P("tp", None, None),
            P("tp", None, None),
            P("tp"),
            P("ep", "tp", None),
            P("ep", "tp", None),
            P(),
            P(),
            P("ep", None),
            P("ep", None),
            P("ep", None, "tp"),
            P("ep", None, "tp"),
            P("ep", "tp", None),
        ),
        out_specs=(P("ep", "tp"), P("ep", "tp", None), P("ep", "tp", None)),
        check_vma=False,
    )
```

```python
import functools
from types import SimpleNamespace

import jax
import jax.numpy as jnp
from jax import lax
from jax.experimental import pallas as pl
from jax.experimental.pallas import tpu as pltpu
from jax.sharding import PartitionSpec as P


def state_step(
    drive,
    real_state,
    imag_state,
    decay_rate,
    frequency,
    log_step,
    input_real,
    input_imag,
    readout_real,
    readout_imaginary,
    passthrough_scale,
):
    highest_precision = lax.Precision.HIGHEST
    count_of_groups, count_of_channels = (input_real.shape[0], input_real.shape[2])
    step = jnp.exp(log_step)[:, None]
    lam_real = -decay_rate
    magnitude = jnp.exp(lam_real * step)
    abar_real = magnitude * jnp.cos(frequency * step)
    abar_imag = magnitude * jnp.sin(frequency * step)
    denom = lam_real * lam_real + frequency * frequency
    numer = abar_real - 1.0
    factor_real = (numer * lam_real + abar_imag * frequency) / denom
    factor_imag = (abar_imag * lam_real - numer * frequency) / denom
    bbar_real = factor_real[..., None] * input_real - factor_imag[..., None] * input_imag
    bbar_imag = factor_real[..., None] * input_imag + factor_imag[..., None] * input_real
    float_values = drive.astype(jnp.float32).reshape(
        drive.shape[0], count_of_groups, count_of_channels
    )
    push_real = jnp.einsum("sgc,gpc->sgp", float_values, bbar_real, precision=highest_precision)
    push_imag = jnp.einsum("sgc,gpc->sgp", float_values, bbar_imag, precision=highest_precision)
    next_state_real = abar_real * real_state - abar_imag * imag_state + push_real
    next_state_imaginary = abar_real * imag_state + abar_imag * real_state + push_imag
    readout_matrix = (
        jnp.einsum("jdr,dyr->jdy", next_state_real, readout_real, precision=highest_precision)
        - jnp.einsum(
            "jdr,dyr->jdy", next_state_imaginary, readout_imaginary, precision=highest_precision
        )
        + passthrough_scale.reshape(count_of_groups, count_of_channels) * float_values
    )
    mixer = jax.nn.gelu(
        readout_matrix.reshape(drive.shape[0], count_of_groups * count_of_channels)
    ).astype(jnp.bfloat16)
    return (mixer, next_state_real, next_state_imaginary)


def slot_table(routes, expert_count, capacity):
    flat = routes.reshape(-1)
    onehot = (flat[:, None] == jnp.arange(expert_count, dtype=jnp.int32)[None, :]).astype(jnp.int32)
    before = jnp.cumsum(onehot, axis=0) - onehot
    slot = jnp.sum(before * onehot, axis=1)
    target = flat * capacity + slot
    return (
        target[None, :] == jnp.arange(expert_count * capacity, dtype=jnp.int32)[:, None]
    ).astype(jnp.bfloat16)


def flipped(index, mask, count):
    other = 0
    bit = 1
    while bit < count:
        digit = lax.rem(lax.div(index, bit), 2)
        other = other + bit * ((1 - digit) if mask & bit else digit)
        bit *= 2
    return other


def dot(left, right):
    return jnp.dot(left, right, preferred_element_type=jnp.float32)


def halves(values):
    high = values.astype(jnp.bfloat16)
    return high, (values - high.astype(jnp.float32)).astype(jnp.bfloat16)


def layer_kernel(ep_count, tp_count, sizes, *refs):
    names_in, names_out, names_scratch = sizes
    r = SimpleNamespace(**dict(zip(names_in + names_out + names_scratch, refs)))
    me_ep, me_tp = lax.axis_index("ep"), lax.axis_index("tp")
    capacity, width = r.out_tok.shape[1], r.out_tok.shape[2]
    channels = r.out_mix.shape[2]
    pairs = ep_count // 2
    slots = ep_count * capacity
    full = width * tp_count
    row_count = r.pieces.shape[1]
    f32, bf16 = jnp.float32, jnp.bfloat16
    tp_of = [flipped(me_tp, p, tp_count) for p in range(tp_count)]
    ep_of = [flipped(me_ep, j, ep_count) for j in range(ep_count)]

    barrier = pltpu.get_barrier_semaphore()
    for p in range(1, tp_count):
        pl.semaphore_signal(
            barrier, inc=1, device_id={"tp": tp_of[p]}, device_id_type=pl.DeviceIdType.MESH
        )
    for j in range(1, ep_count):
        pl.semaphore_signal(
            barrier, inc=1, device_id={"ep": ep_of[j]}, device_id_type=pl.DeviceIdType.MESH
        )

    loads = []

    def load(source, target):
        loads.append(pltpu.make_async_copy(source, target, r.load_sem.at[len(loads)]))
        loads[-1].start()
        return loads[-1]

    load_tokens = load(r.tokens, r.pieces.at[0])
    load_routes = [load(r.choice, r.choice_v), load(r.weight, r.weight_v)]
    load_small = [
        load(r.decay, r.decay_v),
        load(r.freq, r.freq_v),
        load(r.step, r.step_v),
        load(r.pass_, r.pass_v),
        load(r.gain_mix, r.gain_mix_v),
        load(r.gain_ffn, r.gain_ffn_v),
    ]
    load_mats = [
        load(r.in_re, r.in_re_v),
        load(r.in_im, r.in_im_v),
        load(r.re_re, r.re_re_v),
        load(r.re_im, r.re_im_v),
    ]
    load_w_in = load(r.w_in, r.w_in_v)
    load_states = [load(r.state_r, r.state_rv), load(r.state_i, r.state_iv)]
    load_w_out = load(r.w_out, r.w_out_v)
    load_gates = [load(r.gate.at[0], r.gate_v), load(r.up.at[0], r.up_v)]
    load_down = load(r.down.at[0], r.down_v)

    def remote(src, dst, send, recv, **where):
        return pltpu.make_async_remote_copy(
            src_ref=src,
            dst_ref=dst,
            send_sem=send,
            recv_sem=recv,
            device_id=where,
            device_id_type=pl.DeviceIdType.MESH,
        )

    started = []

    def go(copy):
        copy.start()
        started.append(copy)
        return copy

    load_tokens.wait()
    pl.semaphore_wait(barrier, tp_count - 1 + ep_count - 1)
    first = {
        p: go(remote(r.pieces.at[0], r.pieces.at[p], r.a_send.at[p], r.a_recv.at[p],
                     tp=tp_of[p]))
        for p in (3, 1, 2)
    }

    for copy in load_routes:
        copy.wait()
    choice, weight = r.choice_v[...], r.weight_v[...]
    top_count = choice.shape[0]
    experts = lax.broadcasted_iota(jnp.int32, (ep_count, row_count), 0)
    picks = [(choice[k : k + 1] == experts).astype(f32) for k in range(top_count)]
    earlier = (
        lax.broadcasted_iota(jnp.int32, (row_count, row_count), 0)
        < lax.broadcasted_iota(jnp.int32, (row_count, row_count), 1)
    ).astype(bf16)
    before = dot(sum(picks).astype(bf16), earlier)
    spots = lax.broadcasted_iota(jnp.int32, (slots, row_count), 0)
    table, weights = 0.0, 0.0
    for k in range(top_count):
        slot = jnp.sum(before * picks[k], axis=0, keepdims=True).astype(jnp.int32)
        hit = (choice[k : k + 1] * capacity + slot == spots).astype(f32)
        table = table + hit
        weights = weights + hit * weight[k : k + 1]
        before = before + picks[k]
    table = table.astype(bf16)
    r.table[...] = table.reshape(ep_count, capacity, row_count)
    r.out_tok[...] = dot(table, r.pieces[0]).astype(bf16).reshape(ep_count, capacity, width)

    def spread(order, source, arrived, send, recv):
        copies = {}
        for j in order:
            copies[j] = go(remote(source.at[ep_of[j]], arrived.at[0, j], send.at[j], recv.at[j],
                                  ep=ep_of[j]))
        return copies

    tok_z = spread(range(2, ep_count), r.out_tok, r.arr_tok, r.bz_send, r.bz_recv)
    tok_near, tok_far, mix_near, mix_far = {}, {}, {}, {}

    def forward(m, peers, z_copies, arrived, near, send, recv):
        for j in (2 * m, 2 * m + 1):
            z_copies[j].wait_recv()
        block = pl.ds(2 * m, 2)
        for p in peers:
            near[p, m] = go(remote(arrived.at[0, block], arrived.at[p, block], send.at[p, m],
                                   recv.at[p, m], tp=tp_of[p]))

    def tok_forward(m):
        forward(m, (1, 2), tok_z, r.arr_tok, tok_near, r.bn_send, r.bn_recv)

    def tok_relay(m):
        for p in (1, 2):
            tok_near[p, m].wait_recv()
            j = 2 * m + p - 1
            tok_far[p, m] = go(remote(r.arr_tok.at[p, j], r.arr_tok.at[3, j], r.bf_send.at[p, m],
                                      r.bf_recv.at[p, m], tp=tp_of[3 - p]))

    def share(pieces, shared, arrived, send, recv):
        for p in range(tp_count):
            piece = pieces[p]
            arrived[p, 0] = dot(r.table[me_ep], piece).astype(bf16)
            shared[p] = dot(r.table[ep_of[1]], piece).astype(bf16)
        return [
            go(remote(shared.at[p], arrived.at[p, 1], send.at[p], recv.at[p], ep=ep_of[1]))
            for p in range(tp_count)
        ]

    groups = r.decay.shape[0]
    entries = r.in_re_v.shape[1]
    per_group = channels // groups
    eye = (
        lax.broadcasted_iota(jnp.int32, (groups, groups), 0)
        == lax.broadcasted_iota(jnp.int32, (groups, groups), 1)
    ).astype(f32)
    for copy in load_small:
        copy.wait()
    step = jnp.sum(eye * jnp.exp(r.step_v[...]), axis=1, keepdims=True)
    lam = -r.decay_v[...]
    frequency = r.freq_v[...]
    magnitude = jnp.exp(lam * step)
    abar_real = magnitude * jnp.cos(frequency * step)
    abar_imag = magnitude * jnp.sin(frequency * step)
    denom = lam * lam + frequency * frequency
    numer = abar_real - 1.0
    factor_real = (numer * lam + abar_imag * frequency) / denom
    factor_imag = (abar_imag * lam - numer * frequency) / denom

    def per_channel(values):
        return jnp.broadcast_to(values[:, None, :], (groups, per_group, entries)).reshape(
            channels, entries
        )

    wide_real, wide_imag = per_channel(factor_real), per_channel(factor_imag)
    for copy in load_mats:
        copy.wait()
    in_re, in_im = r.in_re_v[...], r.in_im_v[...]
    push_w = jnp.concatenate(
        [wide_real * in_re - wide_imag * in_im, wide_real * in_im + wide_imag * in_re], axis=1
    )
    push_high, push_low = halves(push_w)
    r.push_w[...] = jnp.concatenate([push_high, push_low], axis=1)
    read_w = jnp.concatenate([r.re_re_v[...], -r.re_im_v[...]], axis=1).T
    read_high, read_low = halves(read_w)
    r.read_w[...] = jnp.concatenate([read_high, read_low], axis=0)
    weight_high, weight_low = halves(weights.T)
    r.combine[0], r.combine[1] = weight_high, weight_low
    rows = row_count * groups
    r.replicate[...] = (
        lax.broadcasted_iota(jnp.int32, (rows, row_count), 0) // groups
        == lax.broadcasted_iota(jnp.int32, (rows, row_count), 1)
    ).astype(bf16)
    r.own_group[...] = (
        lax.broadcasted_iota(jnp.int32, (groups, channels), 0)
        == lax.broadcasted_iota(jnp.int32, (groups, channels), 1) // per_group
    ).astype(f32)
    r.abar[0], r.abar[1] = abar_real, abar_imag

    squares, drive = 0.0, None
    early, middle, late = (range(1, pairs)[part] for part in (slice(1), slice(1, 2), slice(2, None)))
    for p in (0, 1, 2, 3):
        if p == 3:
            for m in early:
                tok_forward(m)
        if p:
            first[p].wait_recv()
        piece = r.pieces[p].astype(f32)
        squares = squares + jnp.sum(piece * piece, axis=1, keepdims=True)
        if not p:
            load_w_in.wait()
        term = dot((piece * r.gain_mix_v[tp_of[p]]).astype(bf16), r.w_in_v[tp_of[p]])
        drive = term if drive is None else drive + term
    drive = (drive * lax.rsqrt(squares / full + 1e-06)).astype(bf16)

    for m in middle:
        tok_forward(m)
    spread_drive = dot(r.replicate[...], drive).reshape(row_count, groups, channels)
    spread_drive = (spread_drive * r.own_group[...]).astype(bf16).reshape(rows, channels)
    push = dot(spread_drive, r.push_w[...])
    push = push[:, : 2 * entries] + push[:, 2 * entries :]
    for copy in load_states:
        copy.wait()

    def per_row(values):
        return jnp.broadcast_to(values[None], (row_count, groups, entries)).reshape(rows, entries)

    wide_real, wide_imag = per_row(r.abar[0]), per_row(r.abar[1])
    real, imag = r.state_rv[...], r.state_iv[...]
    next_real = wide_real * real - wide_imag * imag + push[:, :entries]
    next_imag = wide_real * imag + wide_imag * real + push[:, entries:]
    r.next_r[...] = next_real
    r.next_i[...] = next_imag
    both = jnp.concatenate([next_real, next_imag], axis=1).astype(bf16)
    spread_y = dot(jnp.concatenate([both, both], axis=1), r.read_w[...])
    lane_group = lax.broadcasted_iota(jnp.int32, (row_count, 128), 1) // per_group
    lane_groups = 128 // per_group
    readout = []
    for t in range(channels // 128):
        r.spread_y[t] = spread_y[:, t * 128 : (t + 1) * 128]
        picked = None
        for g in range(lane_groups):
            strip = r.spread_y[t, pl.ds(t * lane_groups + g, row_count, groups), :]
            picked = strip if picked is None else jnp.where(lane_group == g, strip, picked)
        readout.append(picked)
    readout = jnp.concatenate(readout, axis=1) + r.pass_v[...] * drive.astype(f32)
    mixer = jax.nn.gelu(readout).astype(bf16)
    r.mixers[0] = mixer

    r.out_mix[...] = dot(table, mixer).astype(bf16).reshape(ep_count, capacity, channels)
    far_first = [j for m in reversed(range(1, pairs)) for j in (2 * m, 2 * m + 1)]
    mix_z = spread(far_first, r.out_mix, r.arr_mix, r.cz_send, r.cz_recv)
    far_half = tuple(reversed(range(pairs // 2, pairs)))
    near_half = tuple(reversed(range(pairs // 2)))
    half = slots // 2
    blocks = ep_count // 2

    def mix_forward(m):
        forward(m, (1, 2, 3), mix_z, r.arr_mix, mix_near, r.cn_send, r.cn_recv)

    for m in late:
        tok_forward(m)
    for m in reversed(far_half[1:]):
        tok_relay(m)
    mix_forward(far_half[0])
    tok_relay(far_half[0])
    for m in far_half[1:]:
        mix_forward(m)
    tok_share = share(r.pieces, r.shared_tok, r.arr_tok, r.bs_send, r.bs_recv)

    def near_traffic():
        copies = {
            p: go(remote(r.mixers.at[0], r.mixers.at[p], r.e_send.at[p], r.e_recv.at[p],
                         tp=tp_of[p]))
            for p in (3, 1, 2)
        }
        for m in near_half[:-1]:
            tok_relay(m)
            mix_forward(m)
        return copies

    mixed = r.mixed

    def mix_rows(chunk, then=None):
        block = pl.ds(2 * chunk[-1], blocks)
        span = pl.ds(2 * chunk[-1] * capacity, half)
        remote_chunk = [m for m in chunk if m]
        early = range(tp_count - 1) if chunk is far_half else ()
        for p in early:
            if p:
                for m in remote_chunk:
                    mix_near[p, m].wait_recv()
            rows_of_p = r.arr_mix[p, block].reshape(half, channels)
            for n in range(tp_count):
                columns = pl.ds(n * width, width)
                term = dot(rows_of_p, r.w_out_v[tp_of[p], :, columns])
                mixed[span, columns] = term if p == 0 else mixed[span, columns] + term
        result = then() if then else None
        for m in remote_chunk:
            for p in (1, 2, 3):
                if p == 3 or not early:
                    mix_near[p, m].wait_recv()
            for p in (1, 2):
                tok_far[p, m].wait_recv()
        rest = [p for p in range(tp_count) if p not in early]
        squares = 0.0
        for n in range(tp_count):
            columns = pl.ds(n * width, width)
            term = mixed[span, columns] if early else 0.0
            for p in rest:
                rows_of_p = r.arr_mix[p, block].reshape(half, channels)
                term = term + dot(rows_of_p, r.w_out_v[tp_of[p], :, columns])
            after = r.arr_tok[tp_of[n], block].reshape(half, width).astype(f32)
            after = (after + term.astype(bf16).astype(f32)).astype(bf16).astype(f32)
            squares = squares + jnp.sum(after * after, axis=1, keepdims=True)
            r.normed[span, columns] = (after * r.gain_ffn_v[n]).astype(bf16)
        scale = lax.rsqrt(squares / full + 1e-06)
        r.scale[span] = jnp.broadcast_to(scale, (half, 128))
        return result

    load_w_out.wait()
    own_mix = mix_rows(far_half, near_traffic)
    for copy in load_gates:
        copy.wait()
    load_down.wait()
    hidden_width = r.hidden.shape[1]
    tile = next(t for t in (512, 256, 128) if hidden_width % t == 0)
    tiles = hidden_width // tile

    def gate_up(first, start, stop):
        span = pl.ds(first, half)

        for n in range(start, stop):
            columns = pl.ds(n * tile, tile)
            scale = r.scale[span, :1]
            gate = dot(r.normed[span], r.gate_v[:, columns]) * scale
            upper = dot(r.normed[span], r.up_v[:, columns]) * scale
            r.hidden[span, columns] = (jax.nn.silu(gate) * upper).astype(bf16)

    def rows_of(j):
        return pl.ds(j * capacity, capacity)

    parts, relay_in, parts_in, held = r.parts, r.relay_in, r.parts_in, r.held
    far_send, pure_send, merged_send = {}, {}, {}

    def down(p, first):
        columns = pl.ds(pl.multiple_of(tp_of[p] * width, width), width)
        return dot(r.hidden[pl.ds(first, half)], r.down_v[:, columns])

    def down_far(first, chunk):
        parts[3, pl.ds(first, half)] = down(3, first).astype(bf16)
        for m in chunk:
            for p in (1, 2):
                j = 2 * m + p - 1
                far_send[p, m] = go(remote(parts.at[3, rows_of(j)], relay_in.at[rows_of(j)],
                                           r.rf_send.at[p, m], r.rf_recv.at[p, m], tp=tp_of[p]))

    def down_near(first, chunk):
        for p in (1, 2):
            value = down(p, first)
            held[p, pl.ds(first, half)] = value
            parts[p, pl.ds(first, half)] = value.astype(bf16)
            for m in chunk:
                j = 2 * m + p - 1
                pure_send[p, m] = go(remote(parts.at[p, rows_of(j)], parts_in.at[p, rows_of(j)],
                                            r.rp_send.at[p, m], r.rp_recv.at[p, m], tp=tp_of[p]))

    def down_own(first):
        held[0, pl.ds(first, half)] = down(0, first)

    def merge(m):
        for p in (1, 2):
            q = 3 - p
            j = 2 * m + p - 1
            far_send[p, m].wait_recv()
            merged = held[q, rows_of(j)] + relay_in[rows_of(j)].astype(f32)
            r.merged[rows_of(j)] = merged.astype(bf16)
            merged_send[q, m] = go(remote(r.merged.at[rows_of(j)], parts_in.at[q, rows_of(j)],
                                          r.rm_send.at[q, m], r.rm_recv.at[q, m], tp=tp_of[q]))

    back = {}

    def finish(m):
        for p in (1, 2):
            pure_send[p, m].wait_recv()
            merged_send[p, m].wait_recv()
        span = pl.ds(2 * m * capacity, 2 * capacity)
        total = held[0, span] + parts_in[1, span].astype(f32) + parts_in[2, span].astype(f32)
        r.results[pl.ds(2 * m, 2)] = total.astype(bf16).reshape(2, capacity, width)
        for j in (2 * m + 1, 2 * m):
            if j:
                back[j] = go(remote(r.results.at[j], r.returned.at[me_ep],
                                    r.z_send.at[j], r.z_recv.at[j], ep=ep_of[j]))

    gate_up(half, 0, tiles)
    for p in (1, 2, 3):
        own_mix[p].wait_recv()
    mix_share = share(r.mixers, r.shared_mix, r.arr_mix, r.cs_send, r.cs_recv)
    down_far(half, far_half)
    down_near(half, far_half)
    down_own(half)
    for copy in tok_share + mix_share:
        copy.wait_recv()
    mix_rows(near_half)
    gate_up(0, 0, tiles // 2)
    for m in far_half:
        merge(m)
    gate_up(0, tiles // 2, tiles)
    down_far(0, near_half)
    down_near(0, near_half)
    for m in far_half:
        finish(m)
    down_own(0)
    for m in near_half:
        merge(m)
    for m in near_half[:-1]:
        finish(m)
    own = pl.ds(pl.multiple_of(me_tp * width, width), width)
    mixed_own = None
    for p in range(tp_count):
        term = dot(r.mixers[p], r.w_out_v[tp_of[p], :, own])
        mixed_own = term if mixed_own is None else mixed_own + term
    after_own = (
        (r.pieces[0].astype(f32) + mixed_own.astype(bf16).astype(f32)).astype(bf16).astype(f32)
    )
    finish(0)
    r.returned[me_ep] = r.results[0]
    for j in range(1, ep_count):
        remote(r.results.at[j], r.returned.at[ep_of[j]], r.z_send.at[j],
               r.z_recv.at[j], ep=ep_of[j]).wait_recv()
    everything = r.returned[...].reshape(slots, width)
    weighted = dot(r.combine[0], everything) + dot(r.combine[1], everything)
    r.out[...] = (after_own + weighted).astype(bf16)
    for copy in started:
        copy.wait_send()


def write_kernel(*refs):
    copies = [pltpu.make_async_copy(refs[k], refs[3 + k], refs[6].at[k]) for k in range(3)]
    for copy in copies:
        copy.start()
    for copy in copies:
        copy.wait()


def layer_call(
    tokens, gain_mix, w_in, decay_rate, frequency, log_step, input_real, input_imag, readout_real,
    readout_imaginary, passthrough_scale, state_real, state_imag, w_out, gain_ffn, expert_choice,
    expert_weight, w_gate, w_up, w_down, capacity, ep_count, tp_count,
):
    row_count, width = tokens.shape
    full = width * tp_count
    groups, entries, per_group = input_real.shape
    channels = groups * per_group
    slots = ep_count * capacity
    pairs = ep_count // 2
    hidden_width = w_gate.shape[2]
    rows = row_count * groups
    bf16, f32 = jnp.bfloat16, jnp.float32
    vmem = pl.BlockSpec(memory_space=pltpu.VMEM)
    hbm = pl.BlockSpec(memory_space=pl.ANY)
    inputs = dict(
        tokens=(tokens, hbm),
        gain_mix=(gain_mix.reshape(tp_count, 1, width), hbm),
        gain_ffn=(gain_ffn.reshape(tp_count, 1, width), hbm),
        decay=(decay_rate, hbm),
        freq=(frequency, hbm),
        step=(log_step.reshape(1, groups), hbm),
        pass_=(passthrough_scale.reshape(1, channels), hbm),
        choice=(expert_choice.T, hbm),
        weight=(expert_weight.T, hbm),
        in_re=(jnp.transpose(input_real, (0, 2, 1)).reshape(channels, entries), hbm),
        in_im=(jnp.transpose(input_imag, (0, 2, 1)).reshape(channels, entries), hbm),
        re_re=(readout_real.reshape(channels, entries), hbm),
        re_im=(readout_imaginary.reshape(channels, entries), hbm),
        state_r=(state_real.reshape(rows, entries), hbm),
        state_i=(state_imag.reshape(rows, entries), hbm),
        w_in=(w_in.reshape(tp_count, width, channels), hbm),
        w_out=(w_out.reshape(tp_count, channels, full), hbm),
        gate=(w_gate, hbm),
        up=(w_up, hbm),
        down=(w_down, hbm),
    )
    outputs = dict(
        out=pltpu.VMEM((row_count, width), bf16),
        next_r=pltpu.VMEM((rows, entries), f32),
        next_i=pltpu.VMEM((rows, entries), f32),
    )
    dma = lambda *shape: pltpu.SemaphoreType.DMA(shape)
    scratch = dict(
        pieces=pltpu.VMEM((tp_count, row_count, width), bf16),
        choice_v=pltpu.VMEM(expert_choice.shape[::-1], expert_choice.dtype),
        weight_v=pltpu.VMEM(expert_weight.shape[::-1], f32),
        decay_v=pltpu.VMEM((groups, entries), f32),
        freq_v=pltpu.VMEM((groups, entries), f32),
        step_v=pltpu.VMEM((1, groups), f32),
        pass_v=pltpu.VMEM((1, channels), f32),
        gain_mix_v=pltpu.VMEM((tp_count, 1, width), f32),
        gain_ffn_v=pltpu.VMEM((tp_count, 1, width), f32),
        table=pltpu.VMEM((ep_count, capacity, row_count), bf16),
        replicate=pltpu.VMEM((rows, row_count), bf16),
        own_group=pltpu.VMEM((groups, channels), f32),
        abar=pltpu.VMEM((2, groups, entries), f32),
        shared_tok=pltpu.VMEM((tp_count, capacity, width), bf16),
        shared_mix=pltpu.VMEM((tp_count, capacity, channels), bf16),
        scale=pltpu.VMEM((slots, 128), f32),
        in_re_v=pltpu.VMEM((channels, entries), f32),
        in_im_v=pltpu.VMEM((channels, entries), f32),
        re_re_v=pltpu.VMEM((channels, entries), f32),
        re_im_v=pltpu.VMEM((channels, entries), f32),
        state_rv=pltpu.VMEM((rows, entries), f32),
        state_iv=pltpu.VMEM((rows, entries), f32),
        w_in_v=pltpu.VMEM((tp_count, width, channels), bf16),
        w_out_v=pltpu.VMEM((tp_count, channels, full), bf16),
        gate_v=pltpu.VMEM((full, hidden_width), bf16),
        up_v=pltpu.VMEM((full, hidden_width), bf16),
        down_v=pltpu.VMEM((hidden_width, full), bf16),
        push_w=pltpu.VMEM((channels, 4 * entries), bf16),
        read_w=pltpu.VMEM((4 * entries, channels), bf16),
        combine=pltpu.VMEM((2, row_count, slots), bf16),
        spread_y=pltpu.VMEM((channels // 128, rows, 128), f32),
        mixers=pltpu.VMEM((tp_count, row_count, channels), bf16),
        out_tok=pltpu.VMEM((ep_count, capacity, width), bf16),
        arr_tok=pltpu.VMEM((tp_count, ep_count, capacity, width), bf16),
        out_mix=pltpu.VMEM((ep_count, capacity, channels), bf16),
        arr_mix=pltpu.VMEM((tp_count, ep_count, capacity, channels), bf16),
        mixed=pltpu.VMEM((slots, full), f32),
        normed=pltpu.VMEM((slots, full), bf16),
        hidden=pltpu.VMEM((slots, hidden_width), bf16),
        parts=pltpu.VMEM((tp_count, slots, width), bf16),
        held=pltpu.VMEM((3, slots, width), f32),
        relay_in=pltpu.VMEM((slots, width), bf16),
        merged=pltpu.VMEM((slots, width), bf16),
        parts_in=pltpu.VMEM((3, slots, width), bf16),
        results=pltpu.VMEM((ep_count, capacity, width), bf16),
        returned=pltpu.VMEM((ep_count, capacity, width), bf16),
        load_sem=dma(20),
    )
    kinds = dict(
        a=(tp_count,), e=(tp_count,), bs=(tp_count,), cs=(tp_count,), bz=(ep_count,), cz=(ep_count,), z=(ep_count,),
        bn=(3, pairs), bf=(3, pairs), cn=(4, pairs),
        rf=(3, pairs), rp=(3, pairs), rm=(3, pairs),
    )
    for name, shape in kinds.items():
        scratch[name + "_send"], scratch[name + "_recv"] = dma(*shape), dma(*shape)
    names = (tuple(inputs), tuple(outputs), tuple(scratch))
    out, next_real, next_imag = pl.pallas_call(
        functools.partial(layer_kernel, ep_count, tp_count, names),
        out_shape=tuple(outputs.values()),
        in_specs=[spec for _, spec in inputs.values()],
        out_specs=(vmem, vmem, vmem),
        scratch_shapes=list(scratch.values()),
        compiler_params=pltpu.CompilerParams(
            collective_id=0, has_side_effects=True, vmem_limit_bytes=60 * 1024 * 1024
        ),
    )(*[value for value, _ in inputs.values()])
    results = [pltpu.with_memory_space_constraint(x, pltpu.VMEM) for x in (out, next_real, next_imag)]
    out, next_real, next_imag = pl.pallas_call(
        write_kernel,
        out_shape=tuple(jax.ShapeDtypeStruct(x.shape, x.dtype) for x in results),
        in_specs=[vmem] * 3,
        out_specs=(hbm, hbm, hbm),
        scratch_shapes=[dma(3)],
    )(*results)
    shape = (row_count, groups, entries)
    return out, next_real.reshape(shape), next_imag.reshape(shape)


def plain_experts(normed, after, table, expert_weight, w_gate, w_up, w_down):
    row_count, top_count = expert_weight.shape
    expert_count = lax.axis_size("ep")
    capacity = table.shape[0] // expert_count
    width = normed.shape[1]
    repeated = jnp.repeat(normed, top_count, axis=0)
    sent = jnp.dot(table, repeated, preferred_element_type=jnp.float32).astype(jnp.bfloat16)
    sent = sent.reshape(expert_count, capacity, width)
    arrived = lax.all_to_all(sent, "ep", split_axis=0, concat_axis=0, tiled=True)
    flat = arrived.reshape(expert_count * capacity, width)
    piece = lax.all_gather(flat, "tp", axis=1, tiled=True)
    gate = jnp.dot(piece, w_gate[0], preferred_element_type=jnp.float32)
    upper = jnp.dot(piece, w_up[0], preferred_element_type=jnp.float32)
    hidden = (jax.nn.silu(gate) * upper).astype(jnp.bfloat16)
    partial_value = jnp.dot(hidden, w_down[0], preferred_element_type=jnp.float32)
    summed = lax.psum_scatter(
        partial_value.astype(jnp.bfloat16), "tp", scatter_dimension=1, tiled=True
    )
    results = summed.reshape(expert_count, capacity, width)
    returned = lax.all_to_all(results, "ep", split_axis=0, concat_axis=0, tiled=True)
    returned = returned.reshape(expert_count * capacity, width)
    picked = jnp.dot(table.T, returned, preferred_element_type=jnp.float32)
    picked = picked.reshape(row_count, top_count, width)
    weighted = jnp.sum(picked * expert_weight[..., None], axis=1)
    return (after.astype(jnp.float32) + weighted).astype(jnp.bfloat16)


def norm(values, gains):
    floats = values.astype(jnp.float32)
    scale = lax.rsqrt(jnp.mean(floats * floats, axis=1, keepdims=True) + 1e-06)
    return (floats * scale * gains).astype(jnp.bfloat16)


def power_of_two(count):
    return count & (count - 1) == 0


def body(
    tokens,
    gain_mix,
    w_in,
    decay_rate,
    frequency,
    log_step,
    input_real,
    input_imag,
    readout_real,
    readout_imaginary,
    passthrough_scale,
    state_real,
    state_imag,
    w_out,
    gain_ffn,
    expert_choice,
    expert_weight,
    w_gate,
    w_up,
    w_down,
):
    tp_count = lax.axis_size("tp")
    expert_count = lax.axis_size("ep")
    row_count, local_width = tokens.shape
    feature_start = lax.axis_index("tp") * local_width
    top_count = expert_choice.shape[1]
    capacity = 2 * row_count * top_count // expert_count
    fused = (
        local_width % 128 == 0
        and w_gate.shape[2] % 128 == 0
        and capacity % 16 == 0
        and tp_count == 4
        and power_of_two(expert_count)
        and 4 <= expert_count <= 8
        and w_in.shape[1] % 128 == 0
        and row_count % 16 == 0
        and input_real.shape[0] % 8 == 0
        and input_real.shape[1] == 64
        and 128 % input_real.shape[2] == 0
    )
    if fused:
        return layer_call(
            tokens,
            gain_mix,
            w_in,
            decay_rate,
            frequency,
            log_step,
            input_real,
            input_imag,
            readout_real,
            readout_imaginary,
            passthrough_scale,
            state_real,
            state_imag,
            w_out,
            gain_ffn,
            expert_choice,
            expert_weight,
            w_gate,
            w_up,
            w_down,
            capacity,
            expert_count,
            tp_count,
        )
    all_tokens = lax.all_gather(tokens, "tp", axis=1, tiled=True)
    drive = jnp.dot(
        norm(all_tokens, gain_mix), w_in, preferred_element_type=jnp.float32
    ).astype(jnp.bfloat16)
    mixer, next_state_real, next_state_imaginary = state_step(
        drive,
        state_real,
        state_imag,
        decay_rate,
        frequency,
        log_step,
        input_real,
        input_imag,
        readout_real,
        readout_imaginary,
        passthrough_scale,
    )
    table = slot_table(expert_choice, expert_count, capacity)
    mixed = jnp.dot(
        lax.all_gather(mixer, "tp", axis=1, tiled=True), w_out, preferred_element_type=jnp.float32
    ).astype(jnp.bfloat16)
    after_all = (all_tokens.astype(jnp.float32) + mixed.astype(jnp.float32)).astype(jnp.bfloat16)
    normed_all = norm(after_all, gain_ffn)
    after = lax.dynamic_slice_in_dim(after_all, feature_start, local_width, 1)
    normed = lax.dynamic_slice_in_dim(normed_all, feature_start, local_width, 1)
    layer_out = plain_experts(normed, after, table, expert_weight, w_gate, w_up, w_down)
    return (layer_out, next_state_real, next_state_imaginary)


def solution(mesh):
    return jax.shard_map(
        body,
        mesh=mesh,
        in_specs=(
            P("ep", "tp"),
            P(),
            P(None, "tp"),
            P("tp", None),
            P("tp", None),
            P("tp"),
            P("tp", None, None),
            P("tp", None, None),
            P("tp", None, None),
            P("tp", None, None),
            P("tp"),
            P("ep", "tp", None),
            P("ep", "tp", None),
            P(),
            P(),
            P("ep", None),
            P("ep", None),
            P("ep", None, "tp"),
            P("ep", None, "tp"),
            P("ep", "tp", None),
        ),
        out_specs=(P("ep", "tp"), P("ep", "tp", None), P("ep", "tp", None)),
        check_vma=False,
    )
```

```python
import functools
import math
from types import SimpleNamespace

import jax
import jax.numpy as jnp
from jax import lax
from jax.experimental import pallas as pl
from jax.experimental.pallas import tpu as pltpu
from jax.sharding import PartitionSpec as P


def state_step(
    drive,
    real_state,
    imag_state,
    decay_rate,
    frequency,
    log_step,
    input_real,
    input_imag,
    readout_real,
    readout_imaginary,
    passthrough_scale,
):
    highest_precision = lax.Precision.HIGHEST
    count_of_groups, count_of_channels = (input_real.shape[0], input_real.shape[2])
    step = jnp.exp(log_step)[:, None]
    lam_real = -decay_rate
    magnitude = jnp.exp(lam_real * step)
    abar_real = magnitude * jnp.cos(frequency * step)
    abar_imag = magnitude * jnp.sin(frequency * step)
    denom = lam_real * lam_real + frequency * frequency
    numer = abar_real - 1.0
    factor_real = (numer * lam_real + abar_imag * frequency) / denom
    factor_imag = (abar_imag * lam_real - numer * frequency) / denom
    bbar_real = factor_real[..., None] * input_real - factor_imag[..., None] * input_imag
    bbar_imag = factor_real[..., None] * input_imag + factor_imag[..., None] * input_real
    float_values = drive.astype(jnp.float32).reshape(
        drive.shape[0], count_of_groups, count_of_channels
    )
    push_real = jnp.einsum("sgc,gpc->sgp", float_values, bbar_real, precision=highest_precision)
    push_imag = jnp.einsum("sgc,gpc->sgp", float_values, bbar_imag, precision=highest_precision)
    next_state_real = abar_real * real_state - abar_imag * imag_state + push_real
    next_state_imaginary = abar_real * imag_state + abar_imag * real_state + push_imag
    readout_matrix = (
        jnp.einsum("jdr,dyr->jdy", next_state_real, readout_real, precision=highest_precision)
        - jnp.einsum(
            "jdr,dyr->jdy", next_state_imaginary, readout_imaginary, precision=highest_precision
        )
        + passthrough_scale.reshape(count_of_groups, count_of_channels) * float_values
    )
    mixer = jax.nn.gelu(
        readout_matrix.reshape(drive.shape[0], count_of_groups * count_of_channels)
    ).astype(jnp.bfloat16)
    return (mixer, next_state_real, next_state_imaginary)


def slot_table(routes, expert_count, capacity):
    flat = routes.reshape(-1)
    onehot = (flat[:, None] == jnp.arange(expert_count, dtype=jnp.int32)[None, :]).astype(jnp.int32)
    before = jnp.cumsum(onehot, axis=0) - onehot
    slot = jnp.sum(before * onehot, axis=1)
    target = flat * capacity + slot
    return (
        target[None, :] == jnp.arange(expert_count * capacity, dtype=jnp.int32)[:, None]
    ).astype(jnp.bfloat16)


def flipped(index, mask, count):
    other = 0
    bit = 1
    while bit < count:
        digit = lax.rem(lax.div(index, bit), 2)
        other = other + bit * ((1 - digit) if mask & bit else digit)
        bit *= 2
    return other


def dot(left, right):
    return jnp.dot(left, right, preferred_element_type=jnp.float32)


def halves(values):
    high = values.astype(jnp.bfloat16)
    return high, (values - high.astype(jnp.float32)).astype(jnp.bfloat16)


def layer_kernel(ep_count, tp_count, sizes, *refs):
    names_in, names_out, names_scratch = sizes
    r = SimpleNamespace(**dict(zip(names_in + names_out + names_scratch, refs)))
    me_ep, me_tp = lax.axis_index("ep"), lax.axis_index("tp")
    capacity, width = r.out_tok.shape[1], r.out_tok.shape[2]
    channels = r.out_mix.shape[2]
    pairs = ep_count // 2
    slots = ep_count * capacity
    full = width * tp_count
    row_count = r.pieces.shape[1]
    f32, bf16 = jnp.float32, jnp.bfloat16
    tp_of = [flipped(me_tp, p, tp_count) for p in range(tp_count)]
    ep_of = [flipped(me_ep, j, ep_count) for j in range(ep_count)]

    barrier = pltpu.get_barrier_semaphore()
    for p in range(1, tp_count):
        pl.semaphore_signal(
            barrier, inc=1, device_id={"tp": tp_of[p]}, device_id_type=pl.DeviceIdType.MESH
        )
    for j in range(1, ep_count):
        pl.semaphore_signal(
            barrier, inc=1, device_id={"ep": ep_of[j]}, device_id_type=pl.DeviceIdType.MESH
        )

    loads = []

    def load(source, target):
        loads.append(pltpu.make_async_copy(source, target, r.load_sem.at[len(loads)]))
        loads[-1].start()
        return loads[-1]

    load_tokens = load(r.tokens, r.pieces.at[0])
    load_routes = [load(r.choice, r.choice_v), load(r.weight, r.weight_v)]
    load_small = [
        load(r.decay, r.decay_v),
        load(r.freq, r.freq_v),
        load(r.step, r.step_v),
        load(r.pass_, r.pass_v),
        load(r.gain_mix, r.gain_mix_v),
        load(r.gain_ffn, r.gain_ffn_v),
    ]
    load_mats = [
        load(r.in_re, r.in_re_v),
        load(r.in_im, r.in_im_v),
        load(r.re_re, r.re_re_v),
        load(r.re_im, r.re_im_v),
    ]
    load_w_in = load(r.w_in, r.w_in_v)
    load_states = [load(r.state_r, r.state_rv), load(r.state_i, r.state_iv)]
    load_w_out = load(r.w_out, r.w_out_v)
    load_gates = [load(r.gate.at[0], r.gate_v), load(r.up.at[0], r.up_v)]
    load_down = load(r.down.at[0], r.down_v)

    def remote(src, dst, recv, **where):
        return pltpu.make_async_remote_copy(
            src_ref=src,
            dst_ref=dst,
            send_sem=r.sent.at[0],
            recv_sem=recv,
            device_id=where,
            device_id_type=pl.DeviceIdType.MESH,
        )

    started = []

    def go(copy):
        copy.start()
        started.append(copy)
        return copy

    def arrive(target, recv):
        remote(target, target, recv, tp=tp_of[1]).wait_recv()

    load_tokens.wait()
    for copy in load_routes:
        copy.wait()
    choice, weight = r.choice_v[...], r.weight_v[...]
    top_count = choice.shape[0]
    experts = lax.broadcasted_iota(jnp.int32, (ep_count, row_count), 0)
    picks = [(choice[k : k + 1] == experts).astype(f32) for k in range(top_count)]
    earlier = (
        lax.broadcasted_iota(jnp.int32, (row_count, row_count), 0)
        < lax.broadcasted_iota(jnp.int32, (row_count, row_count), 1)
    ).astype(bf16)
    before = dot(sum(picks).astype(bf16), earlier)
    spots = lax.broadcasted_iota(jnp.int32, (slots, row_count), 0)
    table, weights = 0.0, 0.0
    for k in range(top_count):
        slot = jnp.sum(before * picks[k], axis=0, keepdims=True).astype(jnp.int32)
        hit = (choice[k : k + 1] * capacity + slot == spots).astype(f32)
        table = table + hit
        weights = weights + hit * weight[k : k + 1]
        before = before + picks[k]
    table = table.astype(bf16)
    r.table[...] = table.reshape(ep_count, capacity, row_count)
    r.out_tok[...] = dot(table, r.pieces[0]).astype(bf16).reshape(ep_count, capacity, width)

    pl.semaphore_wait(barrier, tp_count - 1 + ep_count - 1)
    first = {
        p: go(remote(r.pieces.at[0], r.pieces.at[p], r.a_recv.at[p],
                     tp=tp_of[p]))
        for p in (3, 1, 2)
    }

    def spread(order, source, arrived, recv):
        for j in order:
            go(remote(source.at[ep_of[j]], arrived.at[0, j], recv.at[j // 2], ep=ep_of[j]))

    spread(range(2, ep_count), r.out_tok, r.arr_tok, r.bz_recv)
    def forward(m, peers, arrived, z_recv, recv):
        block = pl.ds(2 * m, 2)
        arrive(arrived.at[0, block], z_recv.at[m])
        for p in peers:
            go(remote(arrived.at[0, block], arrived.at[p, block], recv[p], tp=tp_of[p]))

    def side(m):
        return 0 if m < pairs // 2 else 1

    def tok_forward(m):
        recv = {p: r.bn_recv.at[p - 1, m] for p in (1, 2)}
        forward(m, (1, 2), r.arr_tok, r.bz_recv, recv)

    def tok_relay(m):
        for p in (1, 2):
            arrive(r.arr_tok.at[p, pl.ds(2 * m, 2)], r.bn_recv.at[p - 1, m])
            j = 2 * m + p - 1
            go(remote(r.arr_tok.at[p, j], r.arr_tok.at[3, j], r.bf_recv.at[side(m)],
                      tp=tp_of[3 - p]))

    def share(pieces, shared, arrived, recv):
        for p in range(tp_count):
            piece = pieces[p]
            arrived[p, 0] = dot(r.table[me_ep], piece).astype(bf16)
            shared[p] = dot(r.table[ep_of[1]], piece).astype(bf16)
        for p in range(tp_count):
            go(remote(shared.at[p], arrived.at[p, 1], recv.at[0], ep=ep_of[1]))

    groups = r.decay.shape[0]
    entries = r.in_re_v.shape[1]
    per_group = channels // groups
    eye = (
        lax.broadcasted_iota(jnp.int32, (groups, groups), 0)
        == lax.broadcasted_iota(jnp.int32, (groups, groups), 1)
    ).astype(f32)
    for copy in load_small:
        copy.wait()
    step = jnp.sum(eye * jnp.exp(r.step_v[...]), axis=1, keepdims=True)
    lam = -r.decay_v[...]
    frequency = r.freq_v[...]
    magnitude = jnp.exp(lam * step)
    abar_real = magnitude * jnp.cos(frequency * step)
    abar_imag = magnitude * jnp.sin(frequency * step)
    denom = lam * lam + frequency * frequency
    numer = abar_real - 1.0
    factor_real = (numer * lam + abar_imag * frequency) / denom
    factor_imag = (abar_imag * lam - numer * frequency) / denom

    def per_channel(values):
        return jnp.broadcast_to(values[:, None, :], (groups, per_group, entries)).reshape(
            channels, entries
        )

    wide_real, wide_imag = per_channel(factor_real), per_channel(factor_imag)
    for copy in load_mats:
        copy.wait()
    in_re, in_im = r.in_re_v[...], r.in_im_v[...]
    push_w = jnp.concatenate(
        [wide_real * in_re - wide_imag * in_im, wide_real * in_im + wide_imag * in_re], axis=1
    )
    push_high, push_low = halves(push_w)
    r.push_w[...] = jnp.concatenate([push_high, push_low], axis=1)
    read_w = jnp.concatenate([r.re_re_v[...], -r.re_im_v[...]], axis=1).T
    read_high, read_low = halves(read_w)
    r.read_w[...] = jnp.concatenate([read_high, read_low], axis=0)
    weight_high, weight_low = halves(weights.T)
    r.combine[0], r.combine[1] = weight_high, weight_low
    rows = row_count * groups
    r.replicate[...] = (
        lax.broadcasted_iota(jnp.int32, (rows, row_count), 0) // groups
        == lax.broadcasted_iota(jnp.int32, (rows, row_count), 1)
    ).astype(bf16)
    r.own_group[...] = (
        lax.broadcasted_iota(jnp.int32, (groups, channels), 0)
        == lax.broadcasted_iota(jnp.int32, (groups, channels), 1) // per_group
    ).astype(f32)
    r.abar[0], r.abar[1] = abar_real, abar_imag

    squares, drive = 0.0, None
    early, middle, late = (range(1, pairs)[part] for part in (slice(1), slice(1, 2), slice(2, None)))
    for p in (0, 1, 2, 3):
        if p == 3:
            for m in early:
                tok_forward(m)
        if p:
            first[p].wait_recv()
        piece = r.pieces[p].astype(f32)
        squares = squares + jnp.sum(piece * piece, axis=1, keepdims=True)
        if not p:
            load_w_in.wait()
        term = dot((piece * r.gain_mix_v[tp_of[p]]).astype(bf16), r.w_in_v[tp_of[p]])
        drive = term if drive is None else drive + term
    drive = (drive * lax.rsqrt(squares / full + 1e-06)).astype(bf16)

    spread_drive = dot(r.replicate[...], drive).reshape(row_count, groups, channels)
    spread_drive = (spread_drive * r.own_group[...]).astype(bf16).reshape(rows, channels)
    push = dot(spread_drive, r.push_w[...])
    push = push[:, : 2 * entries] + push[:, 2 * entries :]
    for copy in load_states:
        copy.wait()

    def per_row(values):
        return jnp.broadcast_to(values[None], (row_count, groups, entries)).reshape(rows, entries)

    wide_real, wide_imag = per_row(r.abar[0]), per_row(r.abar[1])
    real, imag = r.state_rv[...], r.state_iv[...]
    next_real = wide_real * real - wide_imag * imag + push[:, :entries]
    next_imag = wide_real * imag + wide_imag * real + push[:, entries:]
    r.next_rv[...] = next_real
    r.next_iv[...] = next_imag
    kept = [
        pltpu.make_async_copy(r.next_rv, r.next_r, r.out_sem.at[0]),
        pltpu.make_async_copy(r.next_iv, r.next_i, r.out_sem.at[1]),
    ]
    for copy in kept:
        copy.start()
    for m in middle:
        tok_forward(m)
    both = jnp.concatenate([next_real, next_imag], axis=1).astype(bf16)
    spread_y = dot(jnp.concatenate([both, both], axis=1), r.read_w[...])
    lane_group = lax.broadcasted_iota(jnp.int32, (row_count, 128), 1) // per_group
    lane_groups = 128 // per_group
    readout = []
    for t in range(channels // 128):
        r.spread_y[t] = spread_y[:, t * 128 : (t + 1) * 128]
        picked = None
        for g in range(lane_groups):
            strip = r.spread_y[t, pl.ds(t * lane_groups + g, row_count, groups), :]
            picked = strip if picked is None else jnp.where(lane_group == g, strip, picked)
        readout.append(picked)
    readout = jnp.concatenate(readout, axis=1) + r.pass_v[...] * drive.astype(f32)
    mixer = jax.nn.gelu(readout).astype(bf16)
    r.mixers[0] = mixer

    r.out_mix[...] = dot(table, mixer).astype(bf16).reshape(ep_count, capacity, channels)
    far_first = [j for m in reversed(range(1, pairs)) for j in (2 * m, 2 * m + 1)]
    spread(far_first, r.out_mix, r.arr_mix, r.cz_recv)
    far_half = tuple(reversed(range(pairs // 2, pairs)))
    near_half = tuple(reversed(range(pairs // 2)))
    half = slots // 2
    blocks = ep_count // 2

    def mix_forward(m):
        recv = {p: r.cn_recv.at[p - 1, side(m)] for p in (1, 2, 3)}
        forward(m, (3, 1, 2), r.arr_mix, r.cz_recv, recv)

    for m in late:
        tok_forward(m)
    for m in reversed(far_half[1:]):
        tok_relay(m)
    mix_forward(far_half[0])
    tok_relay(far_half[0])
    for m in far_half[1:]:
        mix_forward(m)
    share(r.pieces, r.shared_tok, r.arr_tok, r.bs_recv)

    def near_traffic():
        for p in (3, 1, 2):
            go(remote(r.mixers.at[0], r.mixers.at[p], r.e_recv.at[0], tp=tp_of[p]))
        for m in near_half[:-1]:
            tok_relay(m)
            mix_forward(m)

    mixed = r.mixed

    def mix_rows(chunk, then=None):
        block = pl.ds(2 * chunk[-1], blocks)
        span = pl.ds(2 * chunk[-1] * capacity, half)
        remote_chunk = [m for m in chunk if m]
        landed = pl.ds(2 * remote_chunk[-1], 2 * len(remote_chunk))
        early = (0, 3) if chunk is far_half else ()
        for p in early:
            if p:
                arrive(r.arr_mix.at[p, landed], r.cn_recv.at[p - 1, side(chunk[-1])])
            rows_of_p = r.arr_mix[p, block].reshape(half, channels)
            for n in range(tp_count):
                columns = pl.ds(n * width, width)
                term = dot(rows_of_p, r.w_out_v[tp_of[p], :, columns])
                mixed[span, columns] = term if p == 0 else mixed[span, columns] + term
        if then:
            then()
        for p in (1, 2, 3):
            if p not in early:
                arrive(r.arr_mix.at[p, landed], r.cn_recv.at[p - 1, side(chunk[-1])])
        arrive(r.arr_tok.at[3, landed], r.bf_recv.at[side(chunk[-1])])
        rest = [p for p in range(tp_count) if p not in early]
        squares = 0.0
        if not early:
            natural = jnp.concatenate(
                [r.arr_mix[tp_of[n], block].reshape(half, channels) for n in range(tp_count)],
                axis=1,
            )
        for n in range(tp_count):
            columns = pl.ds(n * width, width)
            if early:
                term = mixed[span, columns]
                for p in rest:
                    rows_of_p = r.arr_mix[p, block].reshape(half, channels)
                    term = term + dot(rows_of_p, r.w_out_v[tp_of[p], :, columns])
            else:
                term = dot(natural, r.w_out_v[:, :, columns].reshape(tp_count * channels, width))
            after = r.arr_tok[tp_of[n], block].reshape(half, width).astype(f32)
            after = after + term
            squares = squares + jnp.sum(after * after, axis=1, keepdims=True)
            r.normed[span, columns] = (after * r.gain_ffn_v[n]).astype(bf16)
        scale = lax.rsqrt(squares / full + 1e-06)
        r.scale[span] = jnp.broadcast_to(scale, (half, 128))

    load_w_out.wait()
    mix_rows(far_half, near_traffic)
    for copy in load_gates:
        copy.wait()
    load_down.wait()
    hidden_width = r.hidden.shape[1]
    tile = next(t for t in (512, 256, 128) if hidden_width % t == 0)
    tiles = hidden_width // tile

    def gate_up(first, start, stop):
        span = pl.ds(first, half)

        for n in range(start, stop):
            columns = pl.ds(n * tile, tile)
            scale = r.scale[span, :1]
            gate = dot(r.normed[span], r.gate_v[:, columns]) * scale
            upper = dot(r.normed[span], r.up_v[:, columns]) * scale
            r.hidden[span, columns] = (jax.nn.silu(gate) * upper).astype(bf16)

    def rows_of(j):
        return pl.ds(j * capacity, capacity)

    parts, relay_in, parts_in, held = r.parts, r.relay_in, r.parts_in, r.held

    def down(p, first):
        columns = pl.ds(pl.multiple_of(tp_of[p] * width, width), width)
        return dot(r.hidden[pl.ds(first, half)], r.down_v[:, columns])

    def share_mix():
        arrive(r.mixers.at[pl.ds(1, tp_count - 1)], r.e_recv.at[0])
        share(r.mixers, r.shared_mix, r.arr_mix, r.cs_recv)

    def down_all(first, chunk, midway):
        span = pl.ds(first, half)
        for n in range(tp_count):
            if n == tp_count // 2:
                midway()
            value = dot(r.hidden[span], r.down_v[:, pl.ds(n * width, width)])
            held[n, span] = value
            parts[n, span] = value.astype(bf16)
        send_far(chunk)
        for p in (1, 2):
            send_pure(p, chunk)

    def send_far(chunk):
        for m in chunk:
            for p in (1, 2):
                j = 2 * m + p - 1
                go(remote(parts.at[tp_of[3], rows_of(j)], relay_in.at[rows_of(j)],
                          r.rf_recv.at[m], tp=tp_of[p]))

    def send_pure(p, chunk):
        for m in chunk:
            j = 2 * m + p - 1
            go(remote(parts.at[tp_of[p], rows_of(j)], parts_in.at[p, rows_of(j)],
                      r.rs_recv.at[m], tp=tp_of[p]))

    def down_near(first, chunk):
        span = pl.ds(first, half)
        parts[tp_of[3], span] = down(3, first).astype(bf16)
        send_far(chunk)
        values = [down(p, first) for p in (1, 2)]
        for p, value in zip((1, 2), values):
            held[tp_of[p], span] = value
            parts[tp_of[p], span] = value.astype(bf16)
            send_pure(p, chunk)

    def down_own(first):
        held[tp_of[0], pl.ds(first, half)] = down(0, first)

    def merge(m):
        arrive(relay_in.at[pl.ds(2 * m * capacity, 2 * capacity)], r.rf_recv.at[m])
        for p in (1, 2):
            q = 3 - p
            j = 2 * m + p - 1
            merged = held[tp_of[q], rows_of(j)] + relay_in[rows_of(j)].astype(f32)
            r.merged[rows_of(j)] = merged.astype(bf16)
            go(remote(r.merged.at[rows_of(j)], parts_in.at[q, rows_of(j)], r.rs_recv.at[m],
                      tp=tp_of[q]))

    def finish(m):
        span = pl.ds(2 * m * capacity, 2 * capacity)
        arrive(parts_in.at[pl.ds(1, 2), span], r.rs_recv.at[m])
        total = held[tp_of[0], span] + parts_in[1, span].astype(f32) + parts_in[2, span].astype(f32)
        r.results[pl.ds(2 * m, 2)] = total.astype(bf16).reshape(2, capacity, width)
        for j in (2 * m + 1, 2 * m):
            if j:
                go(remote(r.results.at[j], r.returned.at[me_ep], r.z_recv.at[0], ep=ep_of[j]))

    gate_up(half, 0, tiles)
    down_all(half, far_half, share_mix)
    arrive(r.arr_tok.at[:, 1], r.bs_recv.at[0])
    arrive(r.arr_mix.at[:, 1], r.cs_recv.at[0])
    mix_rows(near_half)
    gate_up(0, 0, tiles // 2)
    for m in far_half:
        merge(m)
    gate_up(0, tiles // 2, tiles)
    down_near(0, near_half)
    for m in far_half:
        finish(m)
    down_own(0)
    own = pl.ds(pl.multiple_of(me_tp * width, width), width)
    mixed_own = None
    for p in range(tp_count):
        term = dot(r.mixers[p], r.w_out_v[tp_of[p], :, own])
        mixed_own = term if mixed_own is None else mixed_own + term
    after_own = (
        (r.pieces[0].astype(f32) + mixed_own.astype(bf16).astype(f32)).astype(bf16).astype(f32)
    )
    for m in near_half:
        merge(m)
    for m in near_half[:-1]:
        finish(m)
    finish(0)
    r.returned[me_ep] = r.results[0]
    arrive(r.results.at[pl.ds(1, ep_count - 1)], r.z_recv.at[0])
    everything = r.returned[...].reshape(slots, width)
    weighted = dot(r.combine[0], everything) + dot(r.combine[1], everything)
    r.out_v[...] = (after_own + weighted).astype(bf16)
    kept.append(pltpu.make_async_copy(r.out_v, r.out, r.out_sem.at[2]))
    kept[-1].start()
    total = sum(2 * math.prod(copy.src_ref.shape) for copy in started)
    sent = r.gate_v.at[pl.ds(0, total // (2 * hidden_width))]
    remote(sent, sent, r.a_recv.at[0], tp=tp_of[1]).wait_send()
    for copy in kept:
        copy.wait()


def write_kernel(*refs):
    copies = [pltpu.make_async_copy(refs[k], refs[3 + k], refs[6].at[k]) for k in range(3)]
    for copy in copies:
        copy.start()
    for copy in copies:
        copy.wait()


def layer_call(
    tokens, gain_mix, w_in, decay_rate, frequency, log_step, input_real, input_imag, readout_real,
    readout_imaginary, passthrough_scale, state_real, state_imag, w_out, gain_ffn, expert_choice,
    expert_weight, w_gate, w_up, w_down, capacity, ep_count, tp_count,
):
    row_count, width = tokens.shape
    full = width * tp_count
    groups, entries, per_group = input_real.shape
    channels = groups * per_group
    slots = ep_count * capacity
    pairs = ep_count // 2
    hidden_width = w_gate.shape[2]
    rows = row_count * groups
    bf16, f32 = jnp.bfloat16, jnp.float32
    vmem = pl.BlockSpec(memory_space=pltpu.VMEM)
    hbm = pl.BlockSpec(memory_space=pl.ANY)
    inputs = dict(
        tokens=(tokens, hbm),
        gain_mix=(gain_mix.reshape(tp_count, 1, width), hbm),
        gain_ffn=(gain_ffn.reshape(tp_count, 1, width), hbm),
        decay=(decay_rate, hbm),
        freq=(frequency, hbm),
        step=(log_step.reshape(1, groups), hbm),
        pass_=(passthrough_scale.reshape(1, channels), hbm),
        choice=(expert_choice.T, hbm),
        weight=(expert_weight.T, hbm),
        in_re=(jnp.transpose(input_real, (0, 2, 1)).reshape(channels, entries), hbm),
        in_im=(jnp.transpose(input_imag, (0, 2, 1)).reshape(channels, entries), hbm),
        re_re=(readout_real.reshape(channels, entries), hbm),
        re_im=(readout_imaginary.reshape(channels, entries), hbm),
        state_r=(state_real.reshape(rows, entries), hbm),
        state_i=(state_imag.reshape(rows, entries), hbm),
        w_in=(w_in.reshape(tp_count, width, channels), hbm),
        w_out=(w_out.reshape(tp_count, channels, full), hbm),
        gate=(w_gate, hbm),
        up=(w_up, hbm),
        down=(w_down, hbm),
    )
    outputs = dict(
        out=pltpu.VMEM((row_count, width), bf16),
        next_r=pltpu.VMEM((rows, entries), f32),
        next_i=pltpu.VMEM((rows, entries), f32),
    )
    dma = lambda *shape: pltpu.SemaphoreType.DMA(shape)
    scratch = dict(
        pieces=pltpu.VMEM((tp_count, row_count, width), bf16),
        choice_v=pltpu.VMEM(expert_choice.shape[::-1], expert_choice.dtype),
        weight_v=pltpu.VMEM(expert_weight.shape[::-1], f32),
        decay_v=pltpu.VMEM((groups, entries), f32),
        freq_v=pltpu.VMEM((groups, entries), f32),
        step_v=pltpu.VMEM((1, groups), f32),
        pass_v=pltpu.VMEM((1, channels), f32),
        gain_mix_v=pltpu.VMEM((tp_count, 1, width), f32),
        gain_ffn_v=pltpu.VMEM((tp_count, 1, width), f32),
        table=pltpu.VMEM((ep_count, capacity, row_count), bf16),
        replicate=pltpu.VMEM((rows, row_count), bf16),
        own_group=pltpu.VMEM((groups, channels), f32),
        abar=pltpu.VMEM((2, groups, entries), f32),
        shared_tok=pltpu.VMEM((tp_count, capacity, width), bf16),
        shared_mix=pltpu.VMEM((tp_count, capacity, channels), bf16),
        scale=pltpu.VMEM((slots, 128), f32),
        in_re_v=pltpu.VMEM((channels, entries), f32),
        in_im_v=pltpu.VMEM((channels, entries), f32),
        re_re_v=pltpu.VMEM((channels, entries), f32),
        re_im_v=pltpu.VMEM((channels, entries), f32),
        state_rv=pltpu.VMEM((rows, entries), f32),
        state_iv=pltpu.VMEM((rows, entries), f32),
        w_in_v=pltpu.VMEM((tp_count, width, channels), bf16),
        w_out_v=pltpu.VMEM((tp_count, channels, full), bf16),
        gate_v=pltpu.VMEM((full, hidden_width), bf16),
        up_v=pltpu.VMEM((full, hidden_width), bf16),
        down_v=pltpu.VMEM((hidden_width, full), bf16),
        push_w=pltpu.VMEM((channels, 4 * entries), bf16),
        read_w=pltpu.VMEM((4 * entries, channels), bf16),
        combine=pltpu.VMEM((2, row_count, slots), bf16),
        spread_y=pltpu.VMEM((channels // 128, rows, 128), f32),
        mixers=pltpu.VMEM((tp_count, row_count, channels), bf16),
        out_tok=pltpu.VMEM((ep_count, capacity, width), bf16),
        arr_tok=pltpu.VMEM((tp_count, ep_count, capacity, width), bf16),
        out_mix=pltpu.VMEM((ep_count, capacity, channels), bf16),
        arr_mix=pltpu.VMEM((tp_count, ep_count, capacity, channels), bf16),
        mixed=pltpu.VMEM((slots, full), f32),
        normed=pltpu.VMEM((slots, full), bf16),
        hidden=pltpu.VMEM((slots, hidden_width), bf16),
        parts=pltpu.VMEM((tp_count, slots, width), bf16),
        held=pltpu.VMEM((tp_count, slots, width), f32),
        relay_in=pltpu.VMEM((slots, width), bf16),
        merged=pltpu.VMEM((slots, width), bf16),
        parts_in=pltpu.VMEM((3, slots, width), bf16),
        results=pltpu.VMEM((ep_count, capacity, width), bf16),
        returned=pltpu.VMEM((ep_count, capacity, width), bf16),
        load_sem=dma(20),
        out_sem=dma(3),
        next_rv=pltpu.VMEM((rows, entries), f32),
        next_iv=pltpu.VMEM((rows, entries), f32),
        out_v=pltpu.VMEM((row_count, width), bf16),
    )
    kinds = dict(
        sent=(1,), a_recv=(tp_count,), e_recv=(1,), bs_recv=(1,), cs_recv=(1,), z_recv=(1,),
        bz_recv=(pairs,), cz_recv=(pairs,), bn_recv=(2, pairs), bf_recv=(2,), cn_recv=(3, 2),
        rf_recv=(pairs,), rs_recv=(pairs,),
    )
    for name, shape in kinds.items():
        scratch[name] = dma(*shape)
    names = (tuple(inputs), tuple(outputs), tuple(scratch))
    out, next_real, next_imag = pl.pallas_call(
        functools.partial(layer_kernel, ep_count, tp_count, names),
        out_shape=tuple(outputs.values()),
        in_specs=[spec for _, spec in inputs.values()],
        out_specs=(hbm, hbm, hbm),
        scratch_shapes=list(scratch.values()),
        compiler_params=pltpu.CompilerParams(
            collective_id=0, has_side_effects=True, vmem_limit_bytes=60 * 1024 * 1024
        ),
    )(*[value for value, _ in inputs.values()])
    results = [pltpu.with_memory_space_constraint(x, pltpu.VMEM) for x in (out, next_real, next_imag)]
    out, next_real, next_imag = pl.pallas_call(
        write_kernel,
        out_shape=tuple(jax.ShapeDtypeStruct(x.shape, x.dtype) for x in results),
        in_specs=[hbm] * 3,
        out_specs=(hbm, hbm, hbm),
        scratch_shapes=[dma(3)],
    )(*results)
    shape = (row_count, groups, entries)
    return out, next_real.reshape(shape), next_imag.reshape(shape)


def plain_experts(normed, after, table, expert_weight, w_gate, w_up, w_down):
    row_count, top_count = expert_weight.shape
    expert_count = lax.axis_size("ep")
    capacity = table.shape[0] // expert_count
    width = normed.shape[1]
    repeated = jnp.repeat(normed, top_count, axis=0)
    sent = jnp.dot(table, repeated, preferred_element_type=jnp.float32).astype(jnp.bfloat16)
    sent = sent.reshape(expert_count, capacity, width)
    arrived = lax.all_to_all(sent, "ep", split_axis=0, concat_axis=0, tiled=True)
    flat = arrived.reshape(expert_count * capacity, width)
    piece = lax.all_gather(flat, "tp", axis=1, tiled=True)
    gate = jnp.dot(piece, w_gate[0], preferred_element_type=jnp.float32)
    upper = jnp.dot(piece, w_up[0], preferred_element_type=jnp.float32)
    hidden = (jax.nn.silu(gate) * upper).astype(jnp.bfloat16)
    partial_value = jnp.dot(hidden, w_down[0], preferred_element_type=jnp.float32)
    summed = lax.psum_scatter(
        partial_value.astype(jnp.bfloat16), "tp", scatter_dimension=1, tiled=True
    )
    results = summed.reshape(expert_count, capacity, width)
    returned = lax.all_to_all(results, "ep", split_axis=0, concat_axis=0, tiled=True)
    returned = returned.reshape(expert_count * capacity, width)
    picked = jnp.dot(table.T, returned, preferred_element_type=jnp.float32)
    picked = picked.reshape(row_count, top_count, width)
    weighted = jnp.sum(picked * expert_weight[..., None], axis=1)
    return (after.astype(jnp.float32) + weighted).astype(jnp.bfloat16)


def norm(values, gains):
    floats = values.astype(jnp.float32)
    scale = lax.rsqrt(jnp.mean(floats * floats, axis=1, keepdims=True) + 1e-06)
    return (floats * scale * gains).astype(jnp.bfloat16)


def power_of_two(count):
    return count & (count - 1) == 0


def body(
    tokens,
    gain_mix,
    w_in,
    decay_rate,
    frequency,
    log_step,
    input_real,
    input_imag,
    readout_real,
    readout_imaginary,
    passthrough_scale,
    state_real,
    state_imag,
    w_out,
    gain_ffn,
    expert_choice,
    expert_weight,
    w_gate,
    w_up,
    w_down,
):
    tp_count = lax.axis_size("tp")
    expert_count = lax.axis_size("ep")
    row_count, local_width = tokens.shape
    feature_start = lax.axis_index("tp") * local_width
    top_count = expert_choice.shape[1]
    capacity = 2 * row_count * top_count // expert_count
    fused = (
        local_width % 128 == 0
        and w_gate.shape[2] % 128 == 0
        and capacity % 16 == 0
        and tp_count == 4
        and power_of_two(expert_count)
        and 4 <= expert_count <= 8
        and w_in.shape[1] % 128 == 0
        and row_count % 16 == 0
        and input_real.shape[0] % 8 == 0
        and input_real.shape[1] == 64
        and 128 % input_real.shape[2] == 0
    )
    if fused:
        return layer_call(
            tokens,
            gain_mix,
            w_in,
            decay_rate,
            frequency,
            log_step,
            input_real,
            input_imag,
            readout_real,
            readout_imaginary,
            passthrough_scale,
            state_real,
            state_imag,
            w_out,
            gain_ffn,
            expert_choice,
            expert_weight,
            w_gate,
            w_up,
            w_down,
            capacity,
            expert_count,
            tp_count,
        )
    all_tokens = lax.all_gather(tokens, "tp", axis=1, tiled=True)
    drive = jnp.dot(
        norm(all_tokens, gain_mix), w_in, preferred_element_type=jnp.float32
    ).astype(jnp.bfloat16)
    mixer, next_state_real, next_state_imaginary = state_step(
        drive,
        state_real,
        state_imag,
        decay_rate,
        frequency,
        log_step,
        input_real,
        input_imag,
        readout_real,
        readout_imaginary,
        passthrough_scale,
    )
    table = slot_table(expert_choice, expert_count, capacity)
    mixed = jnp.dot(
        lax.all_gather(mixer, "tp", axis=1, tiled=True), w_out, preferred_element_type=jnp.float32
    ).astype(jnp.bfloat16)
    after_all = (all_tokens.astype(jnp.float32) + mixed.astype(jnp.float32)).astype(jnp.bfloat16)
    normed_all = norm(after_all, gain_ffn)
    after = lax.dynamic_slice_in_dim(after_all, feature_start, local_width, 1)
    normed = lax.dynamic_slice_in_dim(normed_all, feature_start, local_width, 1)
    layer_out = plain_experts(normed, after, table, expert_weight, w_gate, w_up, w_down)
    return (layer_out, next_state_real, next_state_imaginary)


def solution(mesh):
    return jax.shard_map(
        body,
        mesh=mesh,
        in_specs=(
            P("ep", "tp"),
            P(),
            P(None, "tp"),
            P("tp", None),
            P("tp", None),
            P("tp"),
            P("tp", None, None),
            P("tp", None, None),
            P("tp", None, None),
            P("tp", None, None),
            P("tp"),
            P("ep", "tp", None),
            P("ep", "tp", None),
            P(),
            P(),
            P("ep", None),
            P("ep", None),
            P("ep", None, "tp"),
            P("ep", None, "tp"),
            P("ep", "tp", None),
        ),
        out_specs=(P("ep", "tp"), P("ep", "tp", None), P("ep", "tp", None)),
        check_vma=False,
    )
```

```python
import functools
import math
from types import SimpleNamespace

import jax
import jax.numpy as jnp
from jax import lax
from jax.experimental import pallas as pl
from jax.experimental.pallas import tpu as pltpu
from jax.sharding import PartitionSpec as P


def state_step(
    drive,
    real_state,
    imag_state,
    decay_rate,
    frequency,
    log_step,
    input_real,
    input_imag,
    readout_real,
    readout_imaginary,
    passthrough_scale,
):
    highest_precision = lax.Precision.HIGHEST
    count_of_groups, count_of_channels = (input_real.shape[0], input_real.shape[2])
    step = jnp.exp(log_step)[:, None]
    lam_real = -decay_rate
    magnitude = jnp.exp(lam_real * step)
    abar_real = magnitude * jnp.cos(frequency * step)
    abar_imag = magnitude * jnp.sin(frequency * step)
    denom = lam_real * lam_real + frequency * frequency
    numer = abar_real - 1.0
    factor_real = (numer * lam_real + abar_imag * frequency) / denom
    factor_imag = (abar_imag * lam_real - numer * frequency) / denom
    bbar_real = factor_real[..., None] * input_real - factor_imag[..., None] * input_imag
    bbar_imag = factor_real[..., None] * input_imag + factor_imag[..., None] * input_real
    float_values = drive.astype(jnp.float32).reshape(
        drive.shape[0], count_of_groups, count_of_channels
    )
    push_real = jnp.einsum("sgc,gpc->sgp", float_values, bbar_real, precision=highest_precision)
    push_imag = jnp.einsum("sgc,gpc->sgp", float_values, bbar_imag, precision=highest_precision)
    next_state_real = abar_real * real_state - abar_imag * imag_state + push_real
    next_state_imaginary = abar_real * imag_state + abar_imag * real_state + push_imag
    readout_matrix = (
        jnp.einsum("jdr,dyr->jdy", next_state_real, readout_real, precision=highest_precision)
        - jnp.einsum(
            "jdr,dyr->jdy", next_state_imaginary, readout_imaginary, precision=highest_precision
        )
        + passthrough_scale.reshape(count_of_groups, count_of_channels) * float_values
    )
    mixer = jax.nn.gelu(
        readout_matrix.reshape(drive.shape[0], count_of_groups * count_of_channels)
    ).astype(jnp.bfloat16)
    return (mixer, next_state_real, next_state_imaginary)


def slot_table(routes, expert_count, capacity):
    flat = routes.reshape(-1)
    onehot = (flat[:, None] == jnp.arange(expert_count, dtype=jnp.int32)[None, :]).astype(jnp.int32)
    before = jnp.cumsum(onehot, axis=0) - onehot
    slot = jnp.sum(before * onehot, axis=1)
    target = flat * capacity + slot
    return (
        target[None, :] == jnp.arange(expert_count * capacity, dtype=jnp.int32)[:, None]
    ).astype(jnp.bfloat16)


def flipped(index, mask, count):
    other = 0
    bit = 1
    while bit < count:
        digit = lax.rem(lax.div(index, bit), 2)
        other = other + bit * ((1 - digit) if mask & bit else digit)
        bit *= 2
    return other


def dot(left, right):
    return jnp.dot(left, right, preferred_element_type=jnp.float32)


def halves(values):
    high = values.astype(jnp.bfloat16)
    return high, (values - high.astype(jnp.float32)).astype(jnp.bfloat16)


def layer_kernel(ep_count, tp_count, sizes, *refs):
    names_in, names_out, names_scratch = sizes
    r = SimpleNamespace(**dict(zip(names_in + names_out + names_scratch, refs)))
    me_ep, me_tp = lax.axis_index("ep"), lax.axis_index("tp")
    capacity, width = r.out_tok.shape[1], r.out_tok.shape[2]
    channels = r.out_mix.shape[2]
    pairs = ep_count // 2
    slots = ep_count * capacity
    full = width * tp_count
    row_count = r.pieces.shape[1]
    f32, bf16 = jnp.float32, jnp.bfloat16
    tp_of = [flipped(me_tp, p, tp_count) for p in range(tp_count)]
    ep_of = [flipped(me_ep, j, ep_count) for j in range(ep_count)]

    barrier = pltpu.get_barrier_semaphore()
    for p in range(1, tp_count):
        pl.semaphore_signal(
            barrier, inc=1, device_id={"tp": tp_of[p]}, device_id_type=pl.DeviceIdType.MESH
        )
    for j in range(1, ep_count):
        pl.semaphore_signal(
            barrier, inc=1, device_id={"ep": ep_of[j]}, device_id_type=pl.DeviceIdType.MESH
        )

    loads = []

    def load(*pairs):
        sem = r.load_sem.at[len(loads)]
        for source, target in pairs:
            pltpu.make_async_copy(source, target, sem).start()
        loads.append(sem)
        return sem

    def loaded(target, sem):
        pltpu.make_async_copy(target, target, sem).wait()

    load_tokens = load((r.tokens, r.pieces.at[0]))
    load_choice = load((r.choice, r.choice_v))
    load_weight = load((r.weight, r.weight_v))
    load_poles = load((r.decay, r.poles_v.at[0]), (r.freq, r.poles_v.at[1]))
    load_step = load((r.step, r.step_v))
    load_pass = load((r.pass_, r.pass_v))
    load_gains = load((r.gain_mix, r.gains_v.at[0]), (r.gain_ffn, r.gains_v.at[1]))
    load_mats = load(
        (r.in_re, r.mats_v.at[0]),
        (r.in_im, r.mats_v.at[1]),
        (r.re_re, r.mats_v.at[2]),
        (r.re_im, r.mats_v.at[3]),
    )
    load_w_in = load((r.w_in, r.w_in_v))
    load_states = load((r.state_r, r.states_v.at[0]), (r.state_i, r.states_v.at[1]))
    load_w_out = load((r.w_out, r.w_out_v))
    load_gates = load((r.gate.at[0], r.gates_v.at[0]), (r.up.at[0], r.gates_v.at[1]))
    load_down = load((r.down.at[0], r.down_v))

    def remote(src, dst, recv, **where):
        return pltpu.make_async_remote_copy(
            src_ref=src,
            dst_ref=dst,
            send_sem=r.sent.at[0],
            recv_sem=recv,
            device_id=where,
            device_id_type=pl.DeviceIdType.MESH,
        )

    started = []

    def go(copy):
        copy.start()
        started.append(copy)
        return copy

    def arrive(target, recv):
        remote(target, target, recv, tp=tp_of[1]).wait_recv()

    loaded(r.pieces.at[0], load_tokens)
    loaded(r.choice_v, load_choice)
    loaded(r.weight_v, load_weight)
    choice, weight = r.choice_v[...], r.weight_v[...]
    top_count = choice.shape[0]
    experts = lax.broadcasted_iota(jnp.int32, (ep_count, row_count), 0)
    picks = [(choice[k : k + 1] == experts).astype(f32) for k in range(top_count)]
    earlier = (
        lax.broadcasted_iota(jnp.int32, (row_count, row_count), 0)
        < lax.broadcasted_iota(jnp.int32, (row_count, row_count), 1)
    ).astype(bf16)
    before = dot(sum(picks).astype(bf16), earlier)
    spots = lax.broadcasted_iota(jnp.int32, (slots, row_count), 0)
    table, weights = 0.0, 0.0
    for k in range(top_count):
        slot = jnp.sum(before * picks[k], axis=0, keepdims=True).astype(jnp.int32)
        hit = (choice[k : k + 1] * capacity + slot == spots).astype(f32)
        table = table + hit
        weights = weights + hit * weight[k : k + 1]
        before = before + picks[k]
    table = table.astype(bf16)
    r.table[...] = table.reshape(ep_count, capacity, row_count)
    r.out_tok[...] = dot(table, r.pieces[0]).astype(bf16).reshape(ep_count, capacity, width)

    pl.semaphore_wait(barrier, tp_count - 1 + ep_count - 1)
    first = {
        p: go(remote(r.pieces.at[0], r.pieces.at[p], r.a_recv.at[p],
                     tp=tp_of[p]))
        for p in (3, 1, 2)
    }

    def spread(order, source, arrived, recv):
        for j in order:
            go(remote(source.at[ep_of[j]], arrived.at[0, j], recv.at[j // 2], ep=ep_of[j]))

    spread(range(2, ep_count), r.out_tok, r.arr_tok, r.bz_recv)
    def forward(m, peers, arrived, z_recv, recv):
        block = pl.ds(2 * m, 2)
        arrive(arrived.at[0, block], z_recv.at[m])
        for p in peers:
            go(remote(arrived.at[0, block], arrived.at[p, block], recv[p], tp=tp_of[p]))

    def side(m):
        return 0 if m < pairs // 2 else 1

    def tok_forward(m):
        recv = {p: r.bn_recv.at[p - 1, m] for p in (1, 2)}
        forward(m, (1, 2), r.arr_tok, r.bz_recv, recv)

    def tok_relay(m):
        for p in (1, 2):
            arrive(r.arr_tok.at[p, pl.ds(2 * m, 2)], r.bn_recv.at[p - 1, m])
            j = 2 * m + p - 1
            go(remote(r.arr_tok.at[p, j], r.arr_tok.at[3, j], r.bf_recv.at[side(m)],
                      tp=tp_of[3 - p]))

    def share(pieces, shared, arrived, recv):
        for p in range(tp_count):
            piece = pieces[p]
            arrived[p, 0] = dot(r.table[me_ep], piece).astype(bf16)
            shared[p] = dot(r.table[ep_of[1]], piece).astype(bf16)
        for p in range(tp_count):
            go(remote(shared.at[p], arrived.at[p, 1], recv.at[0], ep=ep_of[1]))

    groups = r.decay.shape[0]
    entries = r.mats_v.shape[2]
    per_group = channels // groups
    eye = (
        lax.broadcasted_iota(jnp.int32, (groups, groups), 0)
        == lax.broadcasted_iota(jnp.int32, (groups, groups), 1)
    ).astype(f32)
    loaded(r.poles_v, load_poles)
    loaded(r.step_v, load_step)
    loaded(r.pass_v, load_pass)
    loaded(r.gains_v, load_gains)
    step = jnp.sum(eye * jnp.exp(r.step_v[...]), axis=1, keepdims=True)
    lam = -r.poles_v[0]
    frequency = r.poles_v[1]
    magnitude = jnp.exp(lam * step)
    abar_real = magnitude * jnp.cos(frequency * step)
    abar_imag = magnitude * jnp.sin(frequency * step)
    denom = lam * lam + frequency * frequency
    numer = abar_real - 1.0
    factor_real = (numer * lam + abar_imag * frequency) / denom
    factor_imag = (abar_imag * lam - numer * frequency) / denom

    def per_channel(values):
        return jnp.broadcast_to(values[:, None, :], (groups, per_group, entries)).reshape(
            channels, entries
        )

    wide_real, wide_imag = per_channel(factor_real), per_channel(factor_imag)
    loaded(r.mats_v, load_mats)
    in_re, in_im = r.mats_v[0], r.mats_v[1]
    push_w = jnp.concatenate(
        [wide_real * in_re - wide_imag * in_im, wide_real * in_im + wide_imag * in_re], axis=1
    )
    push_high, push_low = halves(push_w)
    r.push_w[...] = jnp.concatenate([push_high, push_low], axis=1)
    read_w = jnp.concatenate([r.mats_v[2], -r.mats_v[3]], axis=1).T
    read_high, read_low = halves(read_w)
    r.read_w[...] = jnp.concatenate([read_high, read_low], axis=0)
    weight_high, weight_low = halves(weights.T)
    r.combine[0], r.combine[1] = weight_high, weight_low
    rows = row_count * groups
    r.replicate[...] = (
        lax.broadcasted_iota(jnp.int32, (rows, row_count), 0) // groups
        == lax.broadcasted_iota(jnp.int32, (rows, row_count), 1)
    ).astype(bf16)
    r.own_group[...] = (
        lax.broadcasted_iota(jnp.int32, (groups, channels), 0)
        == lax.broadcasted_iota(jnp.int32, (groups, channels), 1) // per_group
    ).astype(f32)
    r.abar[0], r.abar[1] = abar_real, abar_imag

    squares, drive = 0.0, None
    early, middle, late = (range(1, pairs)[part] for part in (slice(1), slice(1, 2), slice(2, None)))
    for p in (0, 1, 2, 3):
        if p == 3:
            for m in early:
                tok_forward(m)
        if p:
            first[p].wait_recv()
        piece = r.pieces[p].astype(f32)
        squares = squares + jnp.sum(piece * piece, axis=1, keepdims=True)
        if not p:
            loaded(r.w_in_v, load_w_in)
        term = dot((piece * r.gains_v[0, tp_of[p]]).astype(bf16), r.w_in_v[tp_of[p]])
        drive = term if drive is None else drive + term
    drive = (drive * lax.rsqrt(squares / full + 1e-06)).astype(bf16)

    spread_drive = dot(r.replicate[...], drive).reshape(row_count, groups, channels)
    spread_drive = (spread_drive * r.own_group[...]).astype(bf16).reshape(rows, channels)
    push = dot(spread_drive, r.push_w[...])
    push = push[:, : 2 * entries] + push[:, 2 * entries :]
    loaded(r.states_v, load_states)

    def per_row(values):
        return jnp.broadcast_to(values[None], (row_count, groups, entries)).reshape(rows, entries)

    wide_real, wide_imag = per_row(r.abar[0]), per_row(r.abar[1])
    real, imag = r.states_v[0], r.states_v[1]
    next_real = wide_real * real - wide_imag * imag + push[:, :entries]
    next_imag = wide_real * imag + wide_imag * real + push[:, entries:]
    r.next_rv[...] = next_real
    r.next_iv[...] = next_imag
    kept = [
        pltpu.make_async_copy(r.next_rv, r.next_r, r.out_sem.at[0]),
        pltpu.make_async_copy(r.next_iv, r.next_i, r.out_sem.at[1]),
    ]
    for copy in kept:
        copy.start()
    for m in middle:
        tok_forward(m)
    both = jnp.concatenate([next_real, next_imag], axis=1).astype(bf16)
    spread_y = dot(jnp.concatenate([both, both], axis=1), r.read_w[...])
    lane_group = lax.broadcasted_iota(jnp.int32, (row_count, 128), 1) // per_group
    lane_groups = 128 // per_group
    readout = []
    for t in range(channels // 128):
        r.spread_y[t] = spread_y[:, t * 128 : (t + 1) * 128]
        picked = None
        for g in range(lane_groups):
            strip = r.spread_y[t, pl.ds(t * lane_groups + g, row_count, groups), :]
            picked = strip if picked is None else jnp.where(lane_group == g, strip, picked)
        readout.append(picked)
    readout = jnp.concatenate(readout, axis=1) + r.pass_v[...] * drive.astype(f32)
    mixer = jax.nn.gelu(readout).astype(bf16)
    r.mixers[0] = mixer

    r.out_mix[...] = dot(table, mixer).astype(bf16).reshape(ep_count, capacity, channels)
    far_first = [j for m in reversed(range(1, pairs)) for j in (2 * m, 2 * m + 1)]
    spread(far_first, r.out_mix, r.arr_mix, r.cz_recv)
    far_half = tuple(reversed(range(pairs // 2, pairs)))
    near_half = tuple(reversed(range(pairs // 2)))
    half = slots // 2
    blocks = ep_count // 2

    def mix_forward(m):
        recv = {p: r.cn_recv.at[p - 1, side(m)] for p in (1, 2, 3)}
        forward(m, (3, 1, 2), r.arr_mix, r.cz_recv, recv)

    for m in late:
        tok_forward(m)
    for m in reversed(far_half[1:]):
        tok_relay(m)
    mix_forward(far_half[0])
    tok_relay(far_half[0])
    for m in far_half[1:]:
        mix_forward(m)
    share(r.pieces, r.shared_tok, r.arr_tok, r.bs_recv)

    def near_traffic():
        for p in (3, 1, 2):
            go(remote(r.mixers.at[0], r.mixers.at[p], r.e_recv.at[0], tp=tp_of[p]))
        for m in near_half[:-1]:
            tok_relay(m)
            mix_forward(m)

    mixed = r.mixed

    def mix_rows(chunk, then=None):
        block = pl.ds(2 * chunk[-1], blocks)
        span = pl.ds(2 * chunk[-1] * capacity, half)
        remote_chunk = [m for m in chunk if m]
        landed = pl.ds(2 * remote_chunk[-1], 2 * len(remote_chunk))
        early = (0, 3) if chunk is far_half else ()
        for p in early:
            if p:
                arrive(r.arr_mix.at[p, landed], r.cn_recv.at[p - 1, side(chunk[-1])])
            rows_of_p = r.arr_mix[p, block].reshape(half, channels)
            for n in range(tp_count):
                columns = pl.ds(n * width, width)
                term = dot(rows_of_p, r.w_out_v[tp_of[p], :, columns])
                mixed[span, columns] = term if p == 0 else mixed[span, columns] + term
        if then:
            then()
        for p in (1, 2, 3):
            if p not in early:
                arrive(r.arr_mix.at[p, landed], r.cn_recv.at[p - 1, side(chunk[-1])])
        arrive(r.arr_tok.at[3, landed], r.bf_recv.at[side(chunk[-1])])
        rest = [p for p in range(tp_count) if p not in early]
        squares = 0.0
        if not early:
            natural = jnp.concatenate(
                [r.arr_mix[tp_of[n], block].reshape(half, channels) for n in range(tp_count)],
                axis=1,
            )
        for n in range(tp_count):
            columns = pl.ds(n * width, width)
            if early:
                term = mixed[span, columns]
                for p in rest:
                    rows_of_p = r.arr_mix[p, block].reshape(half, channels)
                    term = term + dot(rows_of_p, r.w_out_v[tp_of[p], :, columns])
            else:
                term = dot(natural, r.w_out_v[:, :, columns].reshape(tp_count * channels, width))
            after = r.arr_tok[tp_of[n], block].reshape(half, width).astype(f32)
            after = after + term
            squares = squares + jnp.sum(after * after, axis=1, keepdims=True)
            r.normed[span, columns] = (after * r.gains_v[1, n]).astype(bf16)
        scale = lax.rsqrt(squares / full + 1e-06)
        r.scale[span] = jnp.broadcast_to(scale, (half, 128))

    loaded(r.w_out_v, load_w_out)
    mix_rows(far_half, near_traffic)
    loaded(r.gates_v, load_gates)
    loaded(r.down_v, load_down)
    hidden_width = r.hidden.shape[1]
    tile = next(t for t in (512, 256, 128) if hidden_width % t == 0)
    tiles = hidden_width // tile

    def gate_up(first, start, stop):
        span = pl.ds(first, half)

        for n in range(start, stop):
            columns = pl.ds(n * tile, tile)
            scale = r.scale[span, :1]
            gate = dot(r.normed[span], r.gates_v[0, :, columns]) * scale
            upper = dot(r.normed[span], r.gates_v[1, :, columns]) * scale
            r.hidden[span, columns] = (jax.nn.silu(gate) * upper).astype(bf16)

    def rows_of(j):
        return pl.ds(j * capacity, capacity)

    parts, relay_in, parts_in, held = r.parts, r.relay_in, r.parts_in, r.held

    def down(p, first):
        columns = pl.ds(pl.multiple_of(tp_of[p] * width, width), width)
        return dot(r.hidden[pl.ds(first, half)], r.down_v[:, columns])

    def share_mix():
        arrive(r.mixers.at[pl.ds(1, tp_count - 1)], r.e_recv.at[0])
        share(r.mixers, r.shared_mix, r.arr_mix, r.cs_recv)

    def send_far(chunk):
        for m in chunk:
            for p in (1, 2):
                j = 2 * m + p - 1
                go(remote(parts.at[tp_of[3], rows_of(j)], relay_in.at[rows_of(j)],
                          r.rf_recv.at[m], tp=tp_of[p]))

    def send_pure(p, chunk):
        for m in chunk:
            j = 2 * m + p - 1
            go(remote(parts.at[tp_of[p], rows_of(j)], parts_in.at[p, rows_of(j)],
                      r.rs_recv.at[m], tp=tp_of[p]))

    def down_far(first, chunk):
        parts[tp_of[3], pl.ds(first, half)] = down(3, first).astype(bf16)
        send_far(chunk)

    def down_near(first, chunk):
        span = pl.ds(first, half)
        values = [down(p, first) for p in (1, 2)]
        for p, value in zip((1, 2), values):
            held[tp_of[p], span] = value
            parts[tp_of[p], span] = value.astype(bf16)
            send_pure(p, chunk)

    def down_own(first):
        held[tp_of[0], pl.ds(first, half)] = down(0, first)

    def merge(m):
        arrive(relay_in.at[pl.ds(2 * m * capacity, 2 * capacity)], r.rf_recv.at[m])
        for p in (1, 2):
            q = 3 - p
            j = 2 * m + p - 1
            merged = held[tp_of[q], rows_of(j)] + relay_in[rows_of(j)].astype(f32)
            r.merged[rows_of(j)] = merged.astype(bf16)
            go(remote(r.merged.at[rows_of(j)], parts_in.at[q, rows_of(j)], r.rs_recv.at[m],
                      tp=tp_of[q]))

    def finish(m):
        span = pl.ds(2 * m * capacity, 2 * capacity)
        arrive(parts_in.at[pl.ds(1, 2), span], r.rs_recv.at[m])
        total = held[tp_of[0], span] + parts_in[1, span].astype(f32) + parts_in[2, span].astype(f32)
        r.results[pl.ds(2 * m, 2)] = total.astype(bf16).reshape(2, capacity, width)
        for j in (2 * m + 1, 2 * m):
            if j:
                go(remote(r.results.at[j], r.returned.at[me_ep], r.z_recv.at[0], ep=ep_of[j]))

    gate_up(half, 0, tiles)
    down_far(half, far_half)
    down_near(half, far_half)
    share_mix()
    down_own(half)
    arrive(r.arr_tok.at[:, 1], r.bs_recv.at[0])
    arrive(r.arr_mix.at[:, 1], r.cs_recv.at[0])
    mix_rows(near_half)
    gate_up(0, 0, tiles // 2)
    for m in far_half:
        merge(m)
    gate_up(0, tiles // 2, tiles)
    down_far(0, near_half)
    finish(far_half[0])
    down_near(0, near_half)
    for m in far_half[1:]:
        finish(m)
    down_own(0)
    own = pl.ds(pl.multiple_of(me_tp * width, width), width)
    mixed_own = None
    for p in range(tp_count):
        term = dot(r.mixers[p], r.w_out_v[tp_of[p], :, own])
        mixed_own = term if mixed_own is None else mixed_own + term
    after_own = (
        (r.pieces[0].astype(f32) + mixed_own.astype(bf16).astype(f32)).astype(bf16).astype(f32)
    )
    for m in near_half:
        merge(m)
    for m in near_half[:-1]:
        finish(m)
    finish(0)
    r.returned[me_ep] = r.results[0]
    arrive(r.results.at[pl.ds(1, ep_count - 1)], r.z_recv.at[0])
    everything = r.returned[...].reshape(slots, width)
    weighted = dot(r.combine[0], everything) + dot(r.combine[1], everything)
    r.out[...] = (after_own + weighted).astype(bf16)
    total = sum(2 * math.prod(copy.src_ref.shape) for copy in started)
    sent = r.gates_v.at[0, pl.ds(0, total // (2 * hidden_width))]
    remote(sent, sent, r.a_recv.at[0], tp=tp_of[1]).wait_send()
    for copy in kept:
        copy.wait()


def write_kernel(*refs):
    copies = [pltpu.make_async_copy(refs[k], refs[3 + k], refs[6].at[k]) for k in range(3)]
    for copy in copies:
        copy.start()
    for copy in copies:
        copy.wait()


def layer_call(
    tokens, gain_mix, w_in, decay_rate, frequency, log_step, input_real, input_imag, readout_real,
    readout_imaginary, passthrough_scale, state_real, state_imag, w_out, gain_ffn, expert_choice,
    expert_weight, w_gate, w_up, w_down, capacity, ep_count, tp_count,
):
    row_count, width = tokens.shape
    full = width * tp_count
    groups, entries, per_group = input_real.shape
    channels = groups * per_group
    slots = ep_count * capacity
    pairs = ep_count // 2
    hidden_width = w_gate.shape[2]
    rows = row_count * groups
    bf16, f32 = jnp.bfloat16, jnp.float32
    vmem = pl.BlockSpec(memory_space=pltpu.VMEM)
    hbm = pl.BlockSpec(memory_space=pl.ANY)
    inputs = dict(
        tokens=(tokens, hbm),
        gain_mix=(gain_mix.reshape(tp_count, 1, width), hbm),
        gain_ffn=(gain_ffn.reshape(tp_count, 1, width), hbm),
        decay=(decay_rate, hbm),
        freq=(frequency, hbm),
        step=(log_step.reshape(1, groups), hbm),
        pass_=(passthrough_scale.reshape(1, channels), hbm),
        choice=(expert_choice.T, hbm),
        weight=(expert_weight.T, hbm),
        in_re=(jnp.transpose(input_real, (0, 2, 1)).reshape(channels, entries), hbm),
        in_im=(jnp.transpose(input_imag, (0, 2, 1)).reshape(channels, entries), hbm),
        re_re=(readout_real.reshape(channels, entries), hbm),
        re_im=(readout_imaginary.reshape(channels, entries), hbm),
        state_r=(state_real.reshape(rows, entries), hbm),
        state_i=(state_imag.reshape(rows, entries), hbm),
        w_in=(w_in.reshape(tp_count, width, channels), hbm),
        w_out=(w_out.reshape(tp_count, channels, full), hbm),
        gate=(w_gate, hbm),
        up=(w_up, hbm),
        down=(w_down, hbm),
    )
    outputs = dict(
        out=pltpu.VMEM((row_count, width), bf16),
        next_r=pltpu.VMEM((rows, entries), f32),
        next_i=pltpu.VMEM((rows, entries), f32),
    )
    dma = lambda *shape: pltpu.SemaphoreType.DMA(shape)
    scratch = dict(
        pieces=pltpu.VMEM((tp_count, row_count, width), bf16),
        choice_v=pltpu.VMEM(expert_choice.shape[::-1], expert_choice.dtype),
        weight_v=pltpu.VMEM(expert_weight.shape[::-1], f32),
        poles_v=pltpu.VMEM((2, groups, entries), f32),
        gains_v=pltpu.VMEM((2, tp_count, 1, width), f32),
        mats_v=pltpu.VMEM((4, channels, entries), f32),
        states_v=pltpu.VMEM((2, rows, entries), f32),
        gates_v=pltpu.VMEM((2, full, hidden_width), bf16),
        step_v=pltpu.VMEM((1, groups), f32),
        pass_v=pltpu.VMEM((1, channels), f32),
        table=pltpu.VMEM((ep_count, capacity, row_count), bf16),
        replicate=pltpu.VMEM((rows, row_count), bf16),
        own_group=pltpu.VMEM((groups, channels), f32),
        abar=pltpu.VMEM((2, groups, entries), f32),
        shared_tok=pltpu.VMEM((tp_count, capacity, width), bf16),
        shared_mix=pltpu.VMEM((tp_count, capacity, channels), bf16),
        scale=pltpu.VMEM((slots, 128), f32),
        w_in_v=pltpu.VMEM((tp_count, width, channels), bf16),
        w_out_v=pltpu.VMEM((tp_count, channels, full), bf16),
        down_v=pltpu.VMEM((hidden_width, full), bf16),
        push_w=pltpu.VMEM((channels, 4 * entries), bf16),
        read_w=pltpu.VMEM((4 * entries, channels), bf16),
        combine=pltpu.VMEM((2, row_count, slots), bf16),
        spread_y=pltpu.VMEM((channels // 128, rows, 128), f32),
        mixers=pltpu.VMEM((tp_count, row_count, channels), bf16),
        out_tok=pltpu.VMEM((ep_count, capacity, width), bf16),
        arr_tok=pltpu.VMEM((tp_count, ep_count, capacity, width), bf16),
        out_mix=pltpu.VMEM((ep_count, capacity, channels), bf16),
        arr_mix=pltpu.VMEM((tp_count, ep_count, capacity, channels), bf16),
        mixed=pltpu.VMEM((slots, full), f32),
        normed=pltpu.VMEM((slots, full), bf16),
        hidden=pltpu.VMEM((slots, hidden_width), bf16),
        parts=pltpu.VMEM((tp_count, slots, width), bf16),
        held=pltpu.VMEM((tp_count, slots, width), f32),
        relay_in=pltpu.VMEM((slots, width), bf16),
        merged=pltpu.VMEM((slots, width), bf16),
        parts_in=pltpu.VMEM((3, slots, width), bf16),
        results=pltpu.VMEM((ep_count, capacity, width), bf16),
        returned=pltpu.VMEM((ep_count, capacity, width), bf16),
        load_sem=dma(13),
        out_sem=dma(2),
        next_rv=pltpu.VMEM((rows, entries), f32),
        next_iv=pltpu.VMEM((rows, entries), f32),
    )
    kinds = dict(
        sent=(1,), a_recv=(tp_count,), e_recv=(1,), bs_recv=(1,), cs_recv=(1,), z_recv=(1,),
        bz_recv=(pairs,), cz_recv=(pairs,), bn_recv=(2, pairs), bf_recv=(2,), cn_recv=(3, 2),
        rf_recv=(pairs,), rs_recv=(pairs,),
    )
    for name, shape in kinds.items():
        scratch[name] = dma(*shape)
    names = (tuple(inputs), tuple(outputs), tuple(scratch))
    out, next_real, next_imag = pl.pallas_call(
        functools.partial(layer_kernel, ep_count, tp_count, names),
        out_shape=tuple(outputs.values()),
        in_specs=[spec for _, spec in inputs.values()],
        out_specs=(vmem, hbm, hbm),
        scratch_shapes=list(scratch.values()),
        compiler_params=pltpu.CompilerParams(
            collective_id=0, has_side_effects=True, vmem_limit_bytes=60 * 1024 * 1024
        ),
    )(*[value for value, _ in inputs.values()])
    results = [pltpu.with_memory_space_constraint(x, pltpu.VMEM) for x in (out, next_real, next_imag)]
    out, next_real, next_imag = pl.pallas_call(
        write_kernel,
        out_shape=tuple(jax.ShapeDtypeStruct(x.shape, x.dtype) for x in results),
        in_specs=[hbm] * 3,
        out_specs=(hbm, hbm, hbm),
        scratch_shapes=[dma(3)],
    )(*results)
    shape = (row_count, groups, entries)
    return out, next_real.reshape(shape), next_imag.reshape(shape)


def plain_experts(normed, after, table, expert_weight, w_gate, w_up, w_down):
    row_count, top_count = expert_weight.shape
    expert_count = lax.axis_size("ep")
    capacity = table.shape[0] // expert_count
    width = normed.shape[1]
    repeated = jnp.repeat(normed, top_count, axis=0)
    sent = jnp.dot(table, repeated, preferred_element_type=jnp.float32).astype(jnp.bfloat16)
    sent = sent.reshape(expert_count, capacity, width)
    arrived = lax.all_to_all(sent, "ep", split_axis=0, concat_axis=0, tiled=True)
    flat = arrived.reshape(expert_count * capacity, width)
    piece = lax.all_gather(flat, "tp", axis=1, tiled=True)
    gate = jnp.dot(piece, w_gate[0], preferred_element_type=jnp.float32)
    upper = jnp.dot(piece, w_up[0], preferred_element_type=jnp.float32)
    hidden = (jax.nn.silu(gate) * upper).astype(jnp.bfloat16)
    partial_value = jnp.dot(hidden, w_down[0], preferred_element_type=jnp.float32)
    summed = lax.psum_scatter(
        partial_value.astype(jnp.bfloat16), "tp", scatter_dimension=1, tiled=True
    )
    results = summed.reshape(expert_count, capacity, width)
    returned = lax.all_to_all(results, "ep", split_axis=0, concat_axis=0, tiled=True)
    returned = returned.reshape(expert_count * capacity, width)
    picked = jnp.dot(table.T, returned, preferred_element_type=jnp.float32)
    picked = picked.reshape(row_count, top_count, width)
    weighted = jnp.sum(picked * expert_weight[..., None], axis=1)
    return (after.astype(jnp.float32) + weighted).astype(jnp.bfloat16)


def norm(values, gains):
    floats = values.astype(jnp.float32)
    scale = lax.rsqrt(jnp.mean(floats * floats, axis=1, keepdims=True) + 1e-06)
    return (floats * scale * gains).astype(jnp.bfloat16)


def power_of_two(count):
    return count & (count - 1) == 0


def body(
    tokens,
    gain_mix,
    w_in,
    decay_rate,
    frequency,
    log_step,
    input_real,
    input_imag,
    readout_real,
    readout_imaginary,
    passthrough_scale,
    state_real,
    state_imag,
    w_out,
    gain_ffn,
    expert_choice,
    expert_weight,
    w_gate,
    w_up,
    w_down,
):
    tp_count = lax.axis_size("tp")
    expert_count = lax.axis_size("ep")
    row_count, local_width = tokens.shape
    feature_start = lax.axis_index("tp") * local_width
    top_count = expert_choice.shape[1]
    capacity = 2 * row_count * top_count // expert_count
    fused = (
        local_width % 128 == 0
        and w_gate.shape[2] % 128 == 0
        and capacity % 16 == 0
        and tp_count == 4
        and power_of_two(expert_count)
        and 4 <= expert_count <= 8
        and w_in.shape[1] % 128 == 0
        and row_count % 16 == 0
        and input_real.shape[0] % 8 == 0
        and input_real.shape[1] == 64
        and 128 % input_real.shape[2] == 0
    )
    if fused:
        return layer_call(
            tokens,
            gain_mix,
            w_in,
            decay_rate,
            frequency,
            log_step,
            input_real,
            input_imag,
            readout_real,
            readout_imaginary,
            passthrough_scale,
            state_real,
            state_imag,
            w_out,
            gain_ffn,
            expert_choice,
            expert_weight,
            w_gate,
            w_up,
            w_down,
            capacity,
            expert_count,
            tp_count,
        )
    all_tokens = lax.all_gather(tokens, "tp", axis=1, tiled=True)
    drive = jnp.dot(
        norm(all_tokens, gain_mix), w_in, preferred_element_type=jnp.float32
    ).astype(jnp.bfloat16)
    mixer, next_state_real, next_state_imaginary = state_step(
        drive,
        state_real,
        state_imag,
        decay_rate,
        frequency,
        log_step,
        input_real,
        input_imag,
        readout_real,
        readout_imaginary,
        passthrough_scale,
    )
    table = slot_table(expert_choice, expert_count, capacity)
    mixed = jnp.dot(
        lax.all_gather(mixer, "tp", axis=1, tiled=True), w_out, preferred_element_type=jnp.float32
    ).astype(jnp.bfloat16)
    after_all = (all_tokens.astype(jnp.float32) + mixed.astype(jnp.float32)).astype(jnp.bfloat16)
    normed_all = norm(after_all, gain_ffn)
    after = lax.dynamic_slice_in_dim(after_all, feature_start, local_width, 1)
    normed = lax.dynamic_slice_in_dim(normed_all, feature_start, local_width, 1)
    layer_out = plain_experts(normed, after, table, expert_weight, w_gate, w_up, w_down)
    return (layer_out, next_state_real, next_state_imaginary)


def solution(mesh):
    return jax.shard_map(
        body,
        mesh=mesh,
        in_specs=(
            P("ep", "tp"),
            P(),
            P(None, "tp"),
            P("tp", None),
            P("tp", None),
            P("tp"),
            P("tp", None, None),
            P("tp", None, None),
            P("tp", None, None),
            P("tp", None, None),
            P("tp"),
            P("ep", "tp", None),
            P("ep", "tp", None),
            P(),
            P(),
            P("ep", None),
            P("ep", None),
            P("ep", None, "tp"),
            P("ep", None, "tp"),
            P("ep", "tp", None),
        ),
        out_specs=(P("ep", "tp"), P("ep", "tp", None), P("ep", "tp", None)),
        check_vma=False,
    )
```

```python
import functools
import math
from types import SimpleNamespace

import jax
import jax.numpy as jnp
from jax import lax
from jax.experimental import pallas as pl
from jax.experimental.pallas import tpu as pltpu
from jax.sharding import PartitionSpec as P


def state_step(
    drive,
    real_state,
    imag_state,
    decay_rate,
    frequency,
    log_step,
    input_real,
    input_imag,
    readout_real,
    readout_imaginary,
    passthrough_scale,
):
    highest_precision = lax.Precision.HIGHEST
    count_of_groups, count_of_channels = (input_real.shape[0], input_real.shape[2])
    step = jnp.exp(log_step)[:, None]
    lam_real = -decay_rate
    magnitude = jnp.exp(lam_real * step)
    abar_real = magnitude * jnp.cos(frequency * step)
    abar_imag = magnitude * jnp.sin(frequency * step)
    denom = lam_real * lam_real + frequency * frequency
    numer = abar_real - 1.0
    factor_real = (numer * lam_real + abar_imag * frequency) / denom
    factor_imag = (abar_imag * lam_real - numer * frequency) / denom
    bbar_real = factor_real[..., None] * input_real - factor_imag[..., None] * input_imag
    bbar_imag = factor_real[..., None] * input_imag + factor_imag[..., None] * input_real
    float_values = drive.astype(jnp.float32).reshape(
        drive.shape[0], count_of_groups, count_of_channels
    )
    push_real = jnp.einsum("sgc,gpc->sgp", float_values, bbar_real, precision=highest_precision)
    push_imag = jnp.einsum("sgc,gpc->sgp", float_values, bbar_imag, precision=highest_precision)
    next_state_real = abar_real * real_state - abar_imag * imag_state + push_real
    next_state_imaginary = abar_real * imag_state + abar_imag * real_state + push_imag
    readout_matrix = (
        jnp.einsum("jdr,dyr->jdy", next_state_real, readout_real, precision=highest_precision)
        - jnp.einsum(
            "jdr,dyr->jdy", next_state_imaginary, readout_imaginary, precision=highest_precision
        )
        + passthrough_scale.reshape(count_of_groups, count_of_channels) * float_values
    )
    mixer = jax.nn.gelu(
        readout_matrix.reshape(drive.shape[0], count_of_groups * count_of_channels)
    ).astype(jnp.bfloat16)
    return (mixer, next_state_real, next_state_imaginary)


def slot_table(routes, expert_count, capacity):
    flat = routes.reshape(-1)
    onehot = (flat[:, None] == jnp.arange(expert_count, dtype=jnp.int32)[None, :]).astype(jnp.int32)
    before = jnp.cumsum(onehot, axis=0) - onehot
    slot = jnp.sum(before * onehot, axis=1)
    target = flat * capacity + slot
    return (
        target[None, :] == jnp.arange(expert_count * capacity, dtype=jnp.int32)[:, None]
    ).astype(jnp.bfloat16)


def flipped(index, mask, count):
    other = 0
    bit = 1
    while bit < count:
        digit = lax.rem(lax.div(index, bit), 2)
        other = other + bit * ((1 - digit) if mask & bit else digit)
        bit *= 2
    return other


def dot(left, right):
    return jnp.dot(left, right, preferred_element_type=jnp.float32)


def halves(values):
    high = values.astype(jnp.bfloat16)
    return high, (values - high.astype(jnp.float32)).astype(jnp.bfloat16)


def layer_kernel(ep_count, tp_count, sizes, *refs):
    names_in, names_out, names_scratch = sizes
    r = SimpleNamespace(**dict(zip(names_in + names_out + names_scratch, refs)))
    me_ep, me_tp = lax.axis_index("ep"), lax.axis_index("tp")
    capacity, width = r.out_tok.shape[1], r.out_tok.shape[2]
    channels = r.out_mix.shape[2]
    pairs = ep_count // 2
    slots = ep_count * capacity
    full = width * tp_count
    row_count = r.pieces.shape[1]
    f32, bf16 = jnp.float32, jnp.bfloat16
    tp_of = [flipped(me_tp, p, tp_count) for p in range(tp_count)]
    ep_of = [flipped(me_ep, j, ep_count) for j in range(ep_count)]

    barrier = pltpu.get_barrier_semaphore()
    for p in range(1, tp_count):
        pl.semaphore_signal(
            barrier, inc=1, device_id={"tp": tp_of[p]}, device_id_type=pl.DeviceIdType.MESH
        )
    for j in range(1, ep_count):
        pl.semaphore_signal(
            barrier, inc=1, device_id={"ep": ep_of[j]}, device_id_type=pl.DeviceIdType.MESH
        )

    loads = []

    def load(*pairs):
        sem = r.load_sem.at[len(loads)]
        for source, target in pairs:
            pltpu.make_async_copy(source, target, sem).start()
        loads.append(sem)
        return sem

    def loaded(target, sem):
        pltpu.make_async_copy(target, target, sem).wait()

    load_tokens = load((r.tokens, r.pieces.at[0]))
    load_choice = load((r.choice, r.choice_v))
    load_weight = load((r.weight, r.weight_v))
    load_poles = load((r.decay, r.poles_v.at[0]), (r.freq, r.poles_v.at[1]))
    load_step = load((r.step, r.step_v))
    load_pass = load((r.pass_, r.pass_v))
    load_gains = load((r.gain_mix, r.gains_v.at[0]), (r.gain_ffn, r.gains_v.at[1]))
    load_mats = load(
        (r.in_re, r.mats_v.at[0]),
        (r.in_im, r.mats_v.at[1]),
        (r.re_re, r.mats_v.at[2]),
        (r.re_im, r.mats_v.at[3]),
    )
    load_w_in = load((r.w_in, r.w_in_v))
    load_states = load((r.state_r, r.states_v.at[0]), (r.state_i, r.states_v.at[1]))
    load_w_out = load((r.w_out, r.w_out_v))
    load_gates = load((r.gate.at[0], r.gates_v.at[0]), (r.up.at[0], r.gates_v.at[1]))
    load_down = load((r.down.at[0], r.down_v))

    def remote(src, dst, recv, **where):
        return pltpu.make_async_remote_copy(
            src_ref=src,
            dst_ref=dst,
            send_sem=r.sent.at[0],
            recv_sem=recv,
            device_id=where,
            device_id_type=pl.DeviceIdType.MESH,
        )

    started = []

    def go(copy):
        copy.start()
        started.append(copy)
        return copy

    def arrive(target, recv):
        remote(target, target, recv, tp=tp_of[1]).wait_recv()

    loaded(r.pieces.at[0], load_tokens)
    loaded(r.choice_v, load_choice)
    loaded(r.weight_v, load_weight)
    choice, weight = r.choice_v[...], r.weight_v[...]
    top_count = choice.shape[0]
    experts = lax.broadcasted_iota(jnp.int32, (ep_count, row_count), 0)
    picks = [(choice[k : k + 1] == experts).astype(f32) for k in range(top_count)]
    earlier = (
        lax.broadcasted_iota(jnp.int32, (row_count, row_count), 0)
        < lax.broadcasted_iota(jnp.int32, (row_count, row_count), 1)
    ).astype(bf16)
    before = dot(sum(picks).astype(bf16), earlier)
    spots = lax.broadcasted_iota(jnp.int32, (slots, row_count), 0)
    table, weights = 0.0, 0.0
    for k in range(top_count):
        slot = jnp.sum(before * picks[k], axis=0, keepdims=True).astype(jnp.int32)
        hit = (choice[k : k + 1] * capacity + slot == spots).astype(f32)
        table = table + hit
        weights = weights + hit * weight[k : k + 1]
        before = before + picks[k]
    table = table.astype(bf16)
    r.table[...] = table.reshape(ep_count, capacity, row_count)
    r.out_tok[...] = dot(table, r.pieces[0]).astype(bf16).reshape(ep_count, capacity, width)

    pl.semaphore_wait(barrier, tp_count - 1 + ep_count - 1)
    first = {
        p: go(remote(r.pieces.at[0], r.pieces.at[p], r.a_recv.at[p],
                     tp=tp_of[p]))
        for p in (3, 1, 2)
    }

    def spread(order, source, arrived, recv):
        for j in order:
            go(remote(source.at[ep_of[j]], arrived.at[0, j], recv.at[j // 2], ep=ep_of[j]))

    spread(range(2, ep_count), r.out_tok, r.arr_tok, r.bz_recv)
    def forward(m, peers, arrived, z_recv, recv):
        block = pl.ds(2 * m, 2)
        arrive(arrived.at[0, block], z_recv.at[m])
        for p in peers:
            go(remote(arrived.at[0, block], arrived.at[p, block], recv[p], tp=tp_of[p]))

    def side(m):
        return 0 if m < pairs // 2 else 1

    def tok_forward(m):
        recv = {p: r.bn_recv.at[p - 1, m] for p in (1, 2)}
        forward(m, (1, 2), r.arr_tok, r.bz_recv, recv)

    def tok_relay(m):
        for p in (1, 2):
            arrive(r.arr_tok.at[p, pl.ds(2 * m, 2)], r.bn_recv.at[p - 1, m])
            j = 2 * m + p - 1
            go(remote(r.arr_tok.at[p, j], r.arr_tok.at[3, j], r.bf_recv.at[side(m)],
                      tp=tp_of[3 - p]))

    def share(pieces, shared, arrived, recv):
        for p in range(tp_count):
            piece = pieces[p]
            arrived[p, 0] = dot(r.table[me_ep], piece).astype(bf16)
            shared[p] = dot(r.table[ep_of[1]], piece).astype(bf16)
        for p in range(tp_count):
            go(remote(shared.at[p], arrived.at[p, 1], recv.at[0], ep=ep_of[1]))

    groups = r.decay.shape[0]
    entries = r.mats_v.shape[2]
    per_group = channels // groups
    eye = (
        lax.broadcasted_iota(jnp.int32, (groups, groups), 0)
        == lax.broadcasted_iota(jnp.int32, (groups, groups), 1)
    ).astype(f32)
    loaded(r.poles_v, load_poles)
    loaded(r.step_v, load_step)
    loaded(r.pass_v, load_pass)
    loaded(r.gains_v, load_gains)
    step = jnp.sum(eye * jnp.exp(r.step_v[...]), axis=1, keepdims=True)
    lam = -r.poles_v[0]
    frequency = r.poles_v[1]
    magnitude = jnp.exp(lam * step)
    abar_real = magnitude * jnp.cos(frequency * step)
    abar_imag = magnitude * jnp.sin(frequency * step)
    denom = lam * lam + frequency * frequency
    numer = abar_real - 1.0
    factor_real = (numer * lam + abar_imag * frequency) / denom
    factor_imag = (abar_imag * lam - numer * frequency) / denom

    def per_channel(values):
        return jnp.broadcast_to(values[:, None, :], (groups, per_group, entries)).reshape(
            channels, entries
        )

    wide_real, wide_imag = per_channel(factor_real), per_channel(factor_imag)
    loaded(r.mats_v, load_mats)
    in_re, in_im = r.mats_v[0], r.mats_v[1]
    push_w = jnp.concatenate(
        [wide_real * in_re - wide_imag * in_im, wide_real * in_im + wide_imag * in_re], axis=1
    )
    push_high, push_low = halves(push_w)
    r.push_w[...] = jnp.concatenate([push_high, push_low], axis=1)
    read_w = jnp.concatenate([r.mats_v[2], -r.mats_v[3]], axis=1).T
    read_high, read_low = halves(read_w)
    r.read_w[...] = jnp.concatenate([read_high, read_low], axis=0)
    weight_high, weight_low = halves(weights.T)
    r.combine[0], r.combine[1] = weight_high, weight_low
    rows = row_count * groups
    r.replicate[...] = (
        lax.broadcasted_iota(jnp.int32, (rows, row_count), 0) // groups
        == lax.broadcasted_iota(jnp.int32, (rows, row_count), 1)
    ).astype(bf16)
    r.own_group[...] = (
        lax.broadcasted_iota(jnp.int32, (groups, channels), 0)
        == lax.broadcasted_iota(jnp.int32, (groups, channels), 1) // per_group
    ).astype(f32)
    r.abar[0], r.abar[1] = abar_real, abar_imag

    squares, drive = 0.0, None
    early, middle, late = (range(1, pairs)[part] for part in (slice(1), slice(1, 2), slice(2, None)))
    for p in (0, 1, 2, 3):
        if p == 3:
            for m in early:
                tok_forward(m)
        if p:
            first[p].wait_recv()
        piece = r.pieces[p].astype(f32)
        squares = squares + jnp.sum(piece * piece, axis=1, keepdims=True)
        if not p:
            loaded(r.w_in_v, load_w_in)
        term = dot((piece * r.gains_v[0, tp_of[p]]).astype(bf16), r.w_in_v[tp_of[p]])
        drive = term if drive is None else drive + term
    drive = (drive * lax.rsqrt(squares / full + 1e-06)).astype(bf16)

    spread_drive = dot(r.replicate[...], drive).reshape(row_count, groups, channels)
    spread_drive = (spread_drive * r.own_group[...]).astype(bf16).reshape(rows, channels)
    push = dot(spread_drive, r.push_w[...])
    push = push[:, : 2 * entries] + push[:, 2 * entries :]
    loaded(r.states_v, load_states)

    def per_row(values):
        return jnp.broadcast_to(values[None], (row_count, groups, entries)).reshape(rows, entries)

    wide_real, wide_imag = per_row(r.abar[0]), per_row(r.abar[1])
    real, imag = r.states_v[0], r.states_v[1]
    next_real = wide_real * real - wide_imag * imag + push[:, :entries]
    next_imag = wide_real * imag + wide_imag * real + push[:, entries:]
    r.next_rv[...] = next_real
    r.next_iv[...] = next_imag
    kept = [
        pltpu.make_async_copy(r.next_rv, r.next_r, r.out_sem.at[0]),
        pltpu.make_async_copy(r.next_iv, r.next_i, r.out_sem.at[1]),
    ]
    for copy in kept:
        copy.start()
    for m in middle:
        tok_forward(m)
    both = jnp.concatenate([next_real, next_imag], axis=1).astype(bf16)
    spread_y = dot(jnp.concatenate([both, both], axis=1), r.read_w[...])
    lane_group = lax.broadcasted_iota(jnp.int32, (row_count, 128), 1) // per_group
    lane_groups = 128 // per_group
    readout = []
    for t in range(channels // 128):
        r.spread_y[t] = spread_y[:, t * 128 : (t + 1) * 128]
        picked = None
        for g in range(lane_groups):
            strip = r.spread_y[t, pl.ds(t * lane_groups + g, row_count, groups), :]
            picked = strip if picked is None else jnp.where(lane_group == g, strip, picked)
        readout.append(picked)
    readout = jnp.concatenate(readout, axis=1) + r.pass_v[...] * drive.astype(f32)
    mixer = jax.nn.gelu(readout).astype(bf16)
    r.mixers[0] = mixer

    r.out_mix[...] = dot(table, mixer).astype(bf16).reshape(ep_count, capacity, channels)
    far_first = [j for m in reversed(range(1, pairs)) for j in (2 * m, 2 * m + 1)]
    spread(far_first, r.out_mix, r.arr_mix, r.cz_recv)
    far_half = tuple(reversed(range(pairs // 2, pairs)))
    near_half = tuple(reversed(range(pairs // 2)))
    half = slots // 2
    blocks = ep_count // 2

    def mix_forward(m):
        recv = {p: r.cn_recv.at[p - 1, side(m)] for p in (1, 2, 3)}
        forward(m, (3, 1, 2), r.arr_mix, r.cz_recv, recv)

    for m in late:
        tok_forward(m)
    for m in reversed(far_half[1:]):
        tok_relay(m)
    mix_forward(far_half[0])
    tok_relay(far_half[0])
    for m in far_half[1:]:
        mix_forward(m)
    share(r.pieces, r.shared_tok, r.arr_tok, r.bs_recv)

    def near_traffic():
        for p in (3, 1, 2):
            go(remote(r.mixers.at[0], r.mixers.at[p], r.e_recv.at[0], tp=tp_of[p]))
        for m in near_half[:-1]:
            tok_relay(m)
            mix_forward(m)

    mixed = r.mixed

    def mix_rows(chunk, then=None):
        block = pl.ds(2 * chunk[-1], blocks)
        span = pl.ds(2 * chunk[-1] * capacity, half)
        remote_chunk = [m for m in chunk if m]
        landed = pl.ds(2 * remote_chunk[-1], 2 * len(remote_chunk))
        early = (0, 3) if chunk is far_half else ()
        for p in early:
            if p:
                arrive(r.arr_mix.at[p, landed], r.cn_recv.at[p - 1, side(chunk[-1])])
            rows_of_p = r.arr_mix[p, block].reshape(half, channels)
            for n in range(tp_count):
                columns = pl.ds(n * width, width)
                term = dot(rows_of_p, r.w_out_v[tp_of[p], :, columns])
                mixed[span, columns] = term if p == 0 else mixed[span, columns] + term
        if then:
            then()
        for p in (1, 2, 3):
            if p not in early:
                arrive(r.arr_mix.at[p, landed], r.cn_recv.at[p - 1, side(chunk[-1])])
        arrive(r.arr_tok.at[3, landed], r.bf_recv.at[side(chunk[-1])])
        rest = [p for p in range(tp_count) if p not in early]
        squares = 0.0
        if not early:
            natural = jnp.concatenate(
                [r.arr_mix[tp_of[n], block].reshape(half, channels) for n in range(tp_count)],
                axis=1,
            )
        for n in range(tp_count):
            columns = pl.ds(n * width, width)
            if early:
                term = mixed[span, columns]
                for p in rest:
                    rows_of_p = r.arr_mix[p, block].reshape(half, channels)
                    term = term + dot(rows_of_p, r.w_out_v[tp_of[p], :, columns])
            else:
                term = dot(natural, r.w_out_v[:, :, columns].reshape(tp_count * channels, width))
            after = r.arr_tok[tp_of[n], block].reshape(half, width).astype(f32)
            after = after + term
            squares = squares + jnp.sum(after * after, axis=1, keepdims=True)
            r.normed[span, columns] = (after * r.gains_v[1, n]).astype(bf16)
        scale = lax.rsqrt(squares / full + 1e-06)
        r.scale[span] = jnp.broadcast_to(scale, (half, 128))

    loaded(r.w_out_v, load_w_out)
    mix_rows(far_half, near_traffic)
    loaded(r.gates_v, load_gates)
    loaded(r.down_v, load_down)
    hidden_width = r.hidden.shape[1]
    tile = next(t for t in (1024, 512, 256, 128) if hidden_width % t == 0)
    tiles = hidden_width // tile

    def gate_up(first, start, stop):
        span = pl.ds(first, half)

        for n in range(start, stop):
            columns = pl.ds(n * tile, tile)
            scale = r.scale[span, :1]
            gate = dot(r.normed[span], r.gates_v[0, :, columns]) * scale
            upper = dot(r.normed[span], r.gates_v[1, :, columns]) * scale
            r.hidden[span, columns] = (jax.nn.silu(gate) * upper).astype(bf16)

    def rows_of(j):
        return pl.ds(j * capacity, capacity)

    parts, relay_in, parts_in, held = r.parts, r.relay_in, r.parts_in, r.held

    def down(p, first):
        columns = pl.ds(pl.multiple_of(tp_of[p] * width, width), width)
        return dot(r.hidden[pl.ds(first, half)], r.down_v[:, columns])

    def share_mix():
        arrive(r.mixers.at[pl.ds(1, tp_count - 1)], r.e_recv.at[0])
        share(r.mixers, r.shared_mix, r.arr_mix, r.cs_recv)

    def send_far(chunk):
        for m in chunk:
            for p in (1, 2):
                j = 2 * m + p - 1
                go(remote(parts.at[tp_of[3], rows_of(j)], relay_in.at[rows_of(j)],
                          r.rf_recv.at[m], tp=tp_of[p]))

    def send_pure(p, chunk):
        for m in chunk:
            j = 2 * m + p - 1
            go(remote(parts.at[tp_of[p], rows_of(j)], parts_in.at[p, rows_of(j)],
                      r.rs_recv.at[m], tp=tp_of[p]))

    def down_far(first, chunk):
        parts[tp_of[3], pl.ds(first, half)] = down(3, first).astype(bf16)
        send_far(chunk)

    def down_near(first, chunk):
        span = pl.ds(first, half)
        values = [down(p, first) for p in (1, 2)]
        for p, value in zip((1, 2), values):
            held[tp_of[p], span] = value
            parts[tp_of[p], span] = value.astype(bf16)
            send_pure(p, chunk)

    def down_own(first):
        held[tp_of[0], pl.ds(first, half)] = down(0, first)

    def merge(m):
        arrive(relay_in.at[pl.ds(2 * m * capacity, 2 * capacity)], r.rf_recv.at[m])
        for p in (1, 2):
            q = 3 - p
            j = 2 * m + p - 1
            merged = held[tp_of[q], rows_of(j)] + relay_in[rows_of(j)].astype(f32)
            r.merged[rows_of(j)] = merged.astype(bf16)
            go(remote(r.merged.at[rows_of(j)], parts_in.at[q, rows_of(j)], r.rs_recv.at[m],
                      tp=tp_of[q]))

    def finish(m):
        span = pl.ds(2 * m * capacity, 2 * capacity)
        arrive(parts_in.at[pl.ds(1, 2), span], r.rs_recv.at[m])
        total = held[tp_of[0], span] + parts_in[1, span].astype(f32) + parts_in[2, span].astype(f32)
        r.results[pl.ds(2 * m, 2)] = total.astype(bf16).reshape(2, capacity, width)
        for j in (2 * m + 1, 2 * m):
            if j:
                go(remote(r.results.at[j], r.returned.at[me_ep], r.z_recv.at[0], ep=ep_of[j]))

    gate_up(half, 0, tiles)
    down_far(half, far_half)
    down_near(half, far_half)
    share_mix()
    down_own(half)
    arrive(r.arr_tok.at[:, 1], r.bs_recv.at[0])
    arrive(r.arr_mix.at[:, 1], r.cs_recv.at[0])
    mix_rows(near_half)
    gate_up(0, 0, tiles // 2)
    for m in far_half:
        merge(m)
    gate_up(0, tiles // 2, tiles)
    down_far(0, near_half)
    finish(far_half[0])
    down_near(0, near_half)
    for m in far_half[1:]:
        finish(m)
    down_own(0)
    own = pl.ds(pl.multiple_of(me_tp * width, width), width)
    mixed_own = None
    for p in range(tp_count):
        term = dot(r.mixers[p], r.w_out_v[tp_of[p], :, own])
        mixed_own = term if mixed_own is None else mixed_own + term
    after_own = (
        (r.pieces[0].astype(f32) + mixed_own.astype(bf16).astype(f32)).astype(bf16).astype(f32)
    )
    for m in near_half:
        merge(m)
    for m in near_half[:-1]:
        finish(m)
    finish(0)
    r.returned[me_ep] = r.results[0]
    arrive(r.results.at[pl.ds(1, ep_count - 1)], r.z_recv.at[0])
    everything = r.returned[...].reshape(slots, width)
    weighted = dot(r.combine[0], everything) + dot(r.combine[1], everything)
    r.out[...] = (after_own + weighted).astype(bf16)
    total = sum(2 * math.prod(copy.src_ref.shape) for copy in started)
    sent = r.gates_v.at[0, pl.ds(0, total // (2 * hidden_width))]
    remote(sent, sent, r.a_recv.at[0], tp=tp_of[1]).wait_send()
    for copy in kept:
        copy.wait()


def write_kernel(*refs):
    copies = [pltpu.make_async_copy(refs[k], refs[3 + k], refs[6].at[k]) for k in range(3)]
    for copy in copies:
        copy.start()
    for copy in copies:
        copy.wait()


def layer_call(
    tokens, gain_mix, w_in, decay_rate, frequency, log_step, input_real, input_imag, readout_real,
    readout_imaginary, passthrough_scale, state_real, state_imag, w_out, gain_ffn, expert_choice,
    expert_weight, w_gate, w_up, w_down, capacity, ep_count, tp_count,
):
    row_count, width = tokens.shape
    full = width * tp_count
    groups, entries, per_group = input_real.shape
    channels = groups * per_group
    slots = ep_count * capacity
    pairs = ep_count // 2
    hidden_width = w_gate.shape[2]
    rows = row_count * groups
    bf16, f32 = jnp.bfloat16, jnp.float32
    vmem = pl.BlockSpec(memory_space=pltpu.VMEM)
    hbm = pl.BlockSpec(memory_space=pl.ANY)
    inputs = dict(
        tokens=(tokens, hbm),
        gain_mix=(gain_mix.reshape(tp_count, 1, width), hbm),
        gain_ffn=(gain_ffn.reshape(tp_count, 1, width), hbm),
        decay=(decay_rate, hbm),
        freq=(frequency, hbm),
        step=(log_step.reshape(1, groups), hbm),
        pass_=(passthrough_scale.reshape(1, channels), hbm),
        choice=(expert_choice.T, hbm),
        weight=(expert_weight.T, hbm),
        in_re=(jnp.transpose(input_real, (0, 2, 1)).reshape(channels, entries), hbm),
        in_im=(jnp.transpose(input_imag, (0, 2, 1)).reshape(channels, entries), hbm),
        re_re=(readout_real.reshape(channels, entries), hbm),
        re_im=(readout_imaginary.reshape(channels, entries), hbm),
        state_r=(state_real.reshape(rows, entries), hbm),
        state_i=(state_imag.reshape(rows, entries), hbm),
        w_in=(w_in.reshape(tp_count, width, channels), hbm),
        w_out=(w_out.reshape(tp_count, channels, full), hbm),
        gate=(w_gate, hbm),
        up=(w_up, hbm),
        down=(w_down, hbm),
    )
    outputs = dict(
        out=pltpu.VMEM((row_count, width), bf16),
        next_r=pltpu.VMEM((rows, entries), f32),
        next_i=pltpu.VMEM((rows, entries), f32),
    )
    dma = lambda *shape: pltpu.SemaphoreType.DMA(shape)
    scratch = dict(
        pieces=pltpu.VMEM((tp_count, row_count, width), bf16),
        choice_v=pltpu.VMEM(expert_choice.shape[::-1], expert_choice.dtype),
        weight_v=pltpu.VMEM(expert_weight.shape[::-1], f32),
        poles_v=pltpu.VMEM((2, groups, entries), f32),
        gains_v=pltpu.VMEM((2, tp_count, 1, width), f32),
        mats_v=pltpu.VMEM((4, channels, entries), f32),
        states_v=pltpu.VMEM((2, rows, entries), f32),
        gates_v=pltpu.VMEM((2, full, hidden_width), bf16),
        step_v=pltpu.VMEM((1, groups), f32),
        pass_v=pltpu.VMEM((1, channels), f32),
        table=pltpu.VMEM((ep_count, capacity, row_count), bf16),
        replicate=pltpu.VMEM((rows, row_count), bf16),
        own_group=pltpu.VMEM((groups, channels), f32),
        abar=pltpu.VMEM((2, groups, entries), f32),
        shared_tok=pltpu.VMEM((tp_count, capacity, width), bf16),
        shared_mix=pltpu.VMEM((tp_count, capacity, channels), bf16),
        scale=pltpu.VMEM((slots, 128), f32),
        w_in_v=pltpu.VMEM((tp_count, width, channels), bf16),
        w_out_v=pltpu.VMEM((tp_count, channels, full), bf16),
        down_v=pltpu.VMEM((hidden_width, full), bf16),
        push_w=pltpu.VMEM((channels, 4 * entries), bf16),
        read_w=pltpu.VMEM((4 * entries, channels), bf16),
        combine=pltpu.VMEM((2, row_count, slots), bf16),
        spread_y=pltpu.VMEM((channels // 128, rows, 128), f32),
        mixers=pltpu.VMEM((tp_count, row_count, channels), bf16),
        out_tok=pltpu.VMEM((ep_count, capacity, width), bf16),
        arr_tok=pltpu.VMEM((tp_count, ep_count, capacity, width), bf16),
        out_mix=pltpu.VMEM((ep_count, capacity, channels), bf16),
        arr_mix=pltpu.VMEM((tp_count, ep_count, capacity, channels), bf16),
        mixed=pltpu.VMEM((slots, full), f32),
        normed=pltpu.VMEM((slots, full), bf16),
        hidden=pltpu.VMEM((slots, hidden_width), bf16),
        parts=pltpu.VMEM((tp_count, slots, width), bf16),
        held=pltpu.VMEM((tp_count, slots, width), f32),
        relay_in=pltpu.VMEM((slots, width), bf16),
        merged=pltpu.VMEM((slots, width), bf16),
        parts_in=pltpu.VMEM((3, slots, width), bf16),
        results=pltpu.VMEM((ep_count, capacity, width), bf16),
        returned=pltpu.VMEM((ep_count, capacity, width), bf16),
        load_sem=dma(13),
        out_sem=dma(2),
        next_rv=pltpu.VMEM((rows, entries), f32),
        next_iv=pltpu.VMEM((rows, entries), f32),
    )
    kinds = dict(
        sent=(1,), a_recv=(tp_count,), e_recv=(1,), bs_recv=(1,), cs_recv=(1,), z_recv=(1,),
        bz_recv=(pairs,), cz_recv=(pairs,), bn_recv=(2, pairs), bf_recv=(2,), cn_recv=(3, 2),
        rf_recv=(pairs,), rs_recv=(pairs,),
    )
    for name, shape in kinds.items():
        scratch[name] = dma(*shape)
    names = (tuple(inputs), tuple(outputs), tuple(scratch))
    out, next_real, next_imag = pl.pallas_call(
        functools.partial(layer_kernel, ep_count, tp_count, names),
        out_shape=tuple(outputs.values()),
        in_specs=[spec for _, spec in inputs.values()],
        out_specs=(vmem, hbm, hbm),
        scratch_shapes=list(scratch.values()),
        compiler_params=pltpu.CompilerParams(
            collective_id=0, has_side_effects=True, vmem_limit_bytes=60 * 1024 * 1024
        ),
    )(*[value for value, _ in inputs.values()])
    results = [pltpu.with_memory_space_constraint(x, pltpu.VMEM) for x in (out, next_real, next_imag)]
    out, next_real, next_imag = pl.pallas_call(
        write_kernel,
        out_shape=tuple(jax.ShapeDtypeStruct(x.shape, x.dtype) for x in results),
        in_specs=[hbm] * 3,
        out_specs=(hbm, hbm, hbm),
        scratch_shapes=[dma(3)],
    )(*results)
    shape = (row_count, groups, entries)
    return out, next_real.reshape(shape), next_imag.reshape(shape)


def plain_experts(normed, after, table, expert_weight, w_gate, w_up, w_down):
    row_count, top_count = expert_weight.shape
    expert_count = lax.axis_size("ep")
    capacity = table.shape[0] // expert_count
    width = normed.shape[1]
    repeated = jnp.repeat(normed, top_count, axis=0)
    sent = jnp.dot(table, repeated, preferred_element_type=jnp.float32).astype(jnp.bfloat16)
    sent = sent.reshape(expert_count, capacity, width)
    arrived = lax.all_to_all(sent, "ep", split_axis=0, concat_axis=0, tiled=True)
    flat = arrived.reshape(expert_count * capacity, width)
    piece = lax.all_gather(flat, "tp", axis=1, tiled=True)
    gate = jnp.dot(piece, w_gate[0], preferred_element_type=jnp.float32)
    upper = jnp.dot(piece, w_up[0], preferred_element_type=jnp.float32)
    hidden = (jax.nn.silu(gate) * upper).astype(jnp.bfloat16)
    partial_value = jnp.dot(hidden, w_down[0], preferred_element_type=jnp.float32)
    summed = lax.psum_scatter(
        partial_value.astype(jnp.bfloat16), "tp", scatter_dimension=1, tiled=True
    )
    results = summed.reshape(expert_count, capacity, width)
    returned = lax.all_to_all(results, "ep", split_axis=0, concat_axis=0, tiled=True)
    returned = returned.reshape(expert_count * capacity, width)
    picked = jnp.dot(table.T, returned, preferred_element_type=jnp.float32)
    picked = picked.reshape(row_count, top_count, width)
    weighted = jnp.sum(picked * expert_weight[..., None], axis=1)
    return (after.astype(jnp.float32) + weighted).astype(jnp.bfloat16)


def norm(values, gains):
    floats = values.astype(jnp.float32)
    scale = lax.rsqrt(jnp.mean(floats * floats, axis=1, keepdims=True) + 1e-06)
    return (floats * scale * gains).astype(jnp.bfloat16)


def power_of_two(count):
    return count & (count - 1) == 0


def body(
    tokens,
    gain_mix,
    w_in,
    decay_rate,
    frequency,
    log_step,
    input_real,
    input_imag,
    readout_real,
    readout_imaginary,
    passthrough_scale,
    state_real,
    state_imag,
    w_out,
    gain_ffn,
    expert_choice,
    expert_weight,
    w_gate,
    w_up,
    w_down,
):
    tp_count = lax.axis_size("tp")
    expert_count = lax.axis_size("ep")
    row_count, local_width = tokens.shape
    feature_start = lax.axis_index("tp") * local_width
    top_count = expert_choice.shape[1]
    capacity = 2 * row_count * top_count // expert_count
    fused = (
        local_width % 128 == 0
        and w_gate.shape[2] % 128 == 0
        and capacity % 16 == 0
        and tp_count == 4
        and power_of_two(expert_count)
        and 4 <= expert_count <= 8
        and w_in.shape[1] % 128 == 0
        and row_count % 16 == 0
        and input_real.shape[0] % 8 == 0
        and input_real.shape[1] == 64
        and 128 % input_real.shape[2] == 0
    )
    if fused:
        return layer_call(
            tokens,
            gain_mix,
            w_in,
            decay_rate,
            frequency,
            log_step,
            input_real,
            input_imag,
            readout_real,
            readout_imaginary,
            passthrough_scale,
            state_real,
            state_imag,
            w_out,
            gain_ffn,
            expert_choice,
            expert_weight,
            w_gate,
            w_up,
            w_down,
            capacity,
            expert_count,
            tp_count,
        )
    all_tokens = lax.all_gather(tokens, "tp", axis=1, tiled=True)
    drive = jnp.dot(
        norm(all_tokens, gain_mix), w_in, preferred_element_type=jnp.float32
    ).astype(jnp.bfloat16)
    mixer, next_state_real, next_state_imaginary = state_step(
        drive,
        state_real,
        state_imag,
        decay_rate,
        frequency,
        log_step,
        input_real,
        input_imag,
        readout_real,
        readout_imaginary,
        passthrough_scale,
    )
    table = slot_table(expert_choice, expert_count, capacity)
    mixed = jnp.dot(
        lax.all_gather(mixer, "tp", axis=1, tiled=True), w_out, preferred_element_type=jnp.float32
    ).astype(jnp.bfloat16)
    after_all = (all_tokens.astype(jnp.float32) + mixed.astype(jnp.float32)).astype(jnp.bfloat16)
    normed_all = norm(after_all, gain_ffn)
    after = lax.dynamic_slice_in_dim(after_all, feature_start, local_width, 1)
    normed = lax.dynamic_slice_in_dim(normed_all, feature_start, local_width, 1)
    layer_out = plain_experts(normed, after, table, expert_weight, w_gate, w_up, w_down)
    return (layer_out, next_state_real, next_state_imaginary)


def solution(mesh):
    return jax.shard_map(
        body,
        mesh=mesh,
        in_specs=(
            P("ep", "tp"),
            P(),
            P(None, "tp"),
            P("tp", None),
            P("tp", None),
            P("tp"),
            P("tp", None, None),
            P("tp", None, None),
            P("tp", None, None),
            P("tp", None, None),
            P("tp"),
            P("ep", "tp", None),
            P("ep", "tp", None),
            P(),
            P(),
            P("ep", None),
            P("ep", None),
            P("ep", None, "tp"),
            P("ep", None, "tp"),
            P("ep", "tp", None),
        ),
        out_specs=(P("ep", "tp"), P("ep", "tp", None), P("ep", "tp", None)),
        check_vma=False,
    )
```
